32 devices in a mesh: fs: 4 (over y, x), tp: 8 (over z, core).
Axes of the slice: x: 2, y: 2, z: 4, core: 2. Of those that a mesh axis runs over, the one named last changes fastest.
Arguments:
- tokens: bfloat16 [4096, 2048], P(('fs', 'tp')), may hold values from -6 to 6
- norm_gain: float32 [2048], replicated, may hold values from 0.1 to 1.9
- gate_weight: bfloat16 [2048, 5632], P('fs', 'tp'), may hold values from -0.125 to 0.125
- up_weight: bfloat16 [2048, 5632], P('fs', 'tp'), may hold values from -0.125 to 0.125
- down_weight: bfloat16 [5632, 2048], P('tp', 'fs'), may hold values from -0.078125 to 0.078125
Outputs:
- mixed: bfloat16 [4096, 2048], P(('fs', 'tp'))
The draws below stay inside these ranges and needn't reach their ends.
All inputs are finite; a program needn't handle non-finite values.
Results may differ from the reference program's by a relative error of at most 0.0065.
Values may be sent and summed in bfloat16 or wider, within the bound.
A program may use at most 128 MiB of HBM per device.

```python
import jax
import jax.numpy as jnp
from jax import lax

D = 2048
FF = 5632
TOK_DEV = 128
TOKENS = 4096


def shard_levels(stream_key, extent, pieces, low, high):
    factor_of = 1.0
    for dim, blocks in pieces:
        draws = jax.random.uniform(jax.random.fold_in(jax.random.fold_in(stream_key, 6), dim), (blocks,), jnp.float32, low / len(pieces), high / len(pieces))
        factor_of = factor_of * jnp.repeat(jnp.exp(draws), extent[dim] // blocks).reshape((-1,) + (1,) * (len(extent) - 1 - dim))
    return factor_of


def centred(key, dims, scale, limit, cuts=(), held_as=jnp.bfloat16):
    loudness = shard_levels(key, dims, cuts, -0.22, 0.18) if cuts else 1.0
    entries = jax.random.normal(key, dims, jnp.float32) * scale * loudness
    return jnp.minimum(jnp.maximum(entries, -limit), limit).astype(held_as)


def setup_inputs(seed: int = 0) -> dict:
    streams_of = jax.random.split(jax.random.key(seed), 6)
    return {
        "tokens": centred(streams_of[0], (TOKENS, D), 1.0, 6.0, ((0, 32),)),
        "norm_gain": jnp.clip(1.0 + 0.18 * jax.random.normal(streams_of[1], (D,), jnp.float32), 0.1, 1.9),
        "gate_weight": centred(streams_of[2], (D, FF), D ** -0.5, 0.125, ((0, 4), (1, 8))),
        "up_weight": centred(streams_of[3], (D, FF), D ** -0.5, 0.125, ((0, 4), (1, 8))),
        "down_weight": centred(streams_of[4], (FF, D), FF ** -0.5, 0.078125, ((0, 8), (1, 4))),
    }


eps_floor = 0.05

def reference(tokens, norm_gain, gate_weight, up_weight, down_weight):
    blocks = tokens.reshape(-1, TOK_DEV, D)

    def one_block(rows):
        values = rows.astype(jnp.float32)
        factor = lax.rsqrt(lax.optimization_barrier(jnp.mean(values * values, axis=-1, keepdims=True)) + eps_floor)
        normed = (values * factor * norm_gain).astype(jnp.bfloat16)
        gate = jnp.dot(normed, gate_weight, preferred_element_type=jnp.float32)
        upper = jnp.dot(normed, up_weight, preferred_element_type=jnp.float32)
        hidden = (jax.nn.silu(gate) * upper).astype(jnp.bfloat16)
        return jnp.dot(hidden, down_weight, preferred_element_type=jnp.float32).astype(jnp.bfloat16)
    return lax.map(one_block, blocks).reshape(TOKENS, D)
```

```python
import functools
import math

import jax
import jax.numpy as jnp
from jax import lax
from jax.experimental import pallas as pl
from jax.experimental.pallas import tpu as pltpu

eps_floor = 0.05
MESH = pl.DeviceIdType.MESH
F32 = jnp.float32
BF16 = jnp.bfloat16


def kernel(Y, X, Z, C, cuts, tok, gain, gw, uw, dw, out, nrm, Wg, Wu, Wd, acc_g, acc_u, hid,
           sib_s, sib_r, rs_s, rs_r, part, tok_v, gain_v, w_local,
           w_send, w_recv, t_send, t_recv, ts_send, ts_recv, p_send, p_recv, q_send, q_recv):
    F = Y * X
    f = lax.axis_index("fs")
    t = lax.axis_index("tp")
    y, x = f // X, f % X
    z, c = t // C, t % C
    rows, D = tok.shape
    H, K = gw.shape
    N = dw.shape[1] // cuts
    tile = 2 if Z % 2 == 0 else 1

    def fs_at(j, i):
        return lax.rem(y + j, Y) * X + lax.rem(x + i, X)

    def tp_at(zz, cc):
        return zz * C + cc

    sib = lax.rem(c + 1, C)

    barrier = pltpu.get_barrier_semaphore()
    peers = [{"fs": fs_at(0, i)} for i in range(1, X)] + [{"fs": fs_at(j, 0)} for j in range(1, Y)]
    if C > 1:
        peers += [{"tp": tp_at(z, sib)}]

    def greet(peer):
        pl.semaphore_signal(barrier, inc=1, device_id=peer, device_id_type=MESH)

    for peer in peers:
        greet(peer)
    below, above = jnp.maximum(z - 1, 0), jnp.minimum(z + 1, Z - 1)
    pl.when(z > 0)(lambda: greet({"tp": tp_at(below, c)}))
    pl.when(z < Z - 1)(lambda: greet({"tp": tp_at(above, c)}))

    mats = ((gw, Wg), (uw, Wu), (dw, Wd))
    own_copies = [pltpu.make_async_copy(ref, held.at[f], w_local.at[m]) for m, (ref, held) in enumerate(mats)]
    own_copies += [pltpu.make_async_copy(tok, tok_v, w_local.at[3]), pltpu.make_async_copy(gain, gain_v, w_local.at[4])]
    for cp in own_copies:
        cp.start()

    pl.semaphore_wait(barrier, len(peers) + (z > 0).astype(jnp.int32) + (z < Z - 1).astype(jnp.int32))
    for cp in own_copies:
        cp.wait()

    def piece(m, h, j, i):
        held = mats[m][1].at[fs_at(j, i)]
        if m == 2 and cuts == 2:
            return held.at[:, pl.ds(h * N, N)]
        n = held.shape[0] // 2
        return held.at[pl.ds(h * n, n)]

    def w_copy(m, h, j, i, dj, di):
        slot = ((j - dj) % Y) * X + (i - di) % X
        cp = pltpu.make_async_remote_copy(
            src_ref=piece(m, h, j, i), dst_ref=piece(m, h, j, i),
            send_sem=w_send.at[m], recv_sem=w_recv.at[m, h, slot],
            device_id={"fs": fs_at(dj, di)}, device_id_type=MESH)
        cp.start()

    def w_wait(m, h, j, i):
        ref = piece(m, h, j, i)
        pltpu.make_async_copy(ref, ref, w_recv.at[m, h, j * X + i]).wait()

    def phase_one(ms):
        for m in ms:
            for i in range(1, X):
                w_copy(m, 0, 0, 0, 0, i)
            for j in range(1, Y):
                w_copy(m, 1, 0, 0, j, 0)

    def phase_own(ms):
        for m in ms:
            for i in range(1, X):
                w_copy(m, 1, 0, 0, 0, i)
            for j in range(1, Y):
                w_copy(m, 0, 0, 0, j, 0)

    def phase_relay(ms):
        for m in ms:
            for i in range(1, X):
                w_wait(m, 0, 0, i)
                for j in range(1, Y):
                    w_copy(m, 0, 0, i, j, 0)
            for j in range(1, Y):
                w_wait(m, 1, j, 0)
                for i in range(1, X):
                    w_copy(m, 1, j, 0, 0, i)

    def wait_cross(ms):
        for m in ms:
            for i in range(1, X):
                w_wait(m, 1, 0, i)
            for j in range(1, Y):
                w_wait(m, 0, j, 0)

    def wait_diag(ms):
        for m in ms:
            for j in range(1, Y):
                for i in range(1, X):
                    w_wait(m, 0, j, i)
                    w_wait(m, 1, j, i)

    def tok_chain(direction, s):
        src = z - s if direction == 0 else z + s
        dst = z + 1 if direction == 0 else z - 1
        ok = jnp.logical_and(src >= 0, dst < Z) if direction == 0 else jnp.logical_and(src < Z, dst >= 0)
        src, dst = jnp.clip(src, 0, Z - 1), jnp.clip(dst, 0, Z - 1)
        cp = pltpu.make_async_remote_copy(
            src_ref=nrm.at[c, src], dst_ref=nrm.at[c, src],
            send_sem=t_send.at[direction, s], recv_sem=t_recv.at[direction, s],
            device_id={"tp": tp_at(dst, c)}, device_id_type=MESH)
        return cp, ok

    def tok_sib(zz):
        return pltpu.make_async_remote_copy(
            src_ref=nrm.at[c, zz], dst_ref=nrm.at[c, zz],
            send_sem=ts_send, recv_sem=ts_recv.at[zz],
            device_id={"tp": tp_at(z, sib)}, device_id_type=MESH)

    def tok_start(s):
        for direction in range(2):
            cp, ok = tok_chain(direction, s)
            pl.when(ok)(cp.start)

    def tok_arrive(s):
        for direction in range(2):
            src = z - s if direction == 0 else z + s
            there = src >= 0 if direction == 0 else src < Z
            src = jnp.clip(src, 0, Z - 1)

            @pl.when(there)
            def _():
                pltpu.make_async_copy(nrm.at[c, src], nrm.at[c, src], t_recv.at[direction, s - 1]).wait()
                if C > 1:
                    tok_sib(src).start()

            if s < Z - 1:
                cp, ok = tok_chain(direction, s)
                pl.when(ok)(cp.start)

    phase_one((0, 1))
    values = tok_v[...].astype(F32)
    factor = lax.rsqrt(jnp.mean(values * values, axis=-1, keepdims=True) + eps_floor)
    nrm[c, z] = (values * factor * gain_v[...]).astype(BF16)
    tok_start(0)
    if C > 1:
        tok_sib(z).start()
    phase_own((0, 1))
    if Z > 1:
        tok_arrive(1)
    phase_relay((0, 1))
    for s in range(2, Z):
        tok_arrive(s)
    wait_cross((0, 1))
    phase_one((2,))
    phase_own((2,))
    if C > 1:
        for zz in range(Z):
            ref = nrm.at[sib, zz]
            pltpu.make_async_copy(ref, ref, ts_recv.at[zz]).wait()

    near = [(0, 0)] + [(0, i) for i in range(1, X)] + [(j, 0) for j in range(1, Y)]
    far = [(j, i) for j in range(1, Y) for i in range(1, X)]
    mrows = tile * rows
    per_core = Z // tile

    def product(n, held, group):
        cc, zt = n // per_core, n % per_core
        total = None
        for j, i in group:
            o = fs_at(j, i)
            a = nrm[cc, pl.ds(zt * tile, tile), :, pl.ds(pl.multiple_of(o * K, K), K)].reshape(mrows, K)
            p = lax.dot_general(a, held[o], (((1,), (1,)), ((), ())), preferred_element_type=F32)
            total = p if total is None else total + p
        return total

    @pl.loop(0, C * per_core)
    def _(n):
        acc_g[n] = product(n, Wg, near)
        acc_u[n] = product(n, Wu, near)

    wait_diag((0,))

    @pl.loop(0, C * per_core)
    def _(n):
        g = acc_g[n]
        if far:
            g = g + product(n, Wg, far)
        acc_g[n] = jax.nn.silu(g)

    wait_diag((1,))

    @pl.loop(0, C * per_core)
    def _(n):
        u = acc_u[n]
        if far:
            u = u + product(n, Wu, far)
        hid[n // per_core, pl.ds((n % per_core) * tile, tile)] = (acc_g[n] * u).astype(BF16).reshape(tile, rows, H)

    def sum_slot(direction, d, at):
        return d if direction == 0 else jnp.where(at == d, Z, d)

    def sum_copy(q, direction, d):
        to = above if direction == 0 else below
        return pltpu.make_async_remote_copy(
            src_ref=rs_s.at[q, d], dst_ref=rs_r.at[q, direction, d],
            send_sem=q_send, recv_sem=q_recv.at[q, sum_slot(direction, d, to)],
            device_id={"tp": tp_at(to, c)}, device_id_type=MESH)

    def sum_wait(q, direction, d):
        ref = rs_r.at[q, direction, d]
        pltpu.make_async_copy(ref, ref, q_recv.at[q, sum_slot(direction, d, z)]).wait()

    units = []

    def down(new):
        qs = list(range(len(units), len(units) + len(new)))
        units.extend(new)

        def weight(q):
            j, i, h = units[q]
            return Wd[fs_at(j, i), :, h * N:(h + 1) * N]

        copies = []
        if C > 1:
            for q in qs:
                sib_s[q] = jnp.dot(hid[sib].reshape(Z * rows, H), weight(q),
                                   preferred_element_type=F32).astype(BF16).reshape(Z, rows, N)
                cp = pltpu.make_async_remote_copy(
                    src_ref=sib_s.at[q], dst_ref=sib_r.at[q], send_sem=p_send, recv_sem=p_recv.at[q],
                    device_id={"tp": tp_at(z, sib)}, device_id_type=MESH)
                cp.start()
                copies.append(cp)
        for q in qs:
            part[q] = jnp.dot(hid[c].reshape(Z * rows, H), weight(q),
                              preferred_element_type=F32).reshape(Z, rows, N)
        for q, cp in zip(qs, copies):
            cp.wait_recv()

            @pl.loop(0, Z)
            def _(d):
                part[q, d] = part[q, d] + sib_r[q, d].astype(F32)

        for direction, first, order in ((0, z == 0, range(Z - 1, 0, -1)), (1, z == Z - 1, range(Z - 1))):
            @pl.when(first)
            def _():
                for d in order:
                    for q in qs:
                        rs_s[q, d] = part[q, d].astype(BF16)
                        sum_copy(q, direction, d).start()
        return qs

    low = 2 * z < Z

    def sum_step(q, direction, d, ok):
        @pl.when(ok)
        def _():
            sum_wait(q, direction, d)
            rs_s[q, d] = (part[q, d] + rs_r[q, direction, d].astype(F32)).astype(BF16)
            sum_copy(q, direction, d).start()

    def sum_near(qs):
        for d in range(Z - 1, 0, -1):
            for q in qs:
                sum_step(q, 0, d, jnp.logical_and(jnp.logical_and(z > 0, z < d), low))
        for d in range(Z - 1):
            for q in qs:
                sum_step(q, 1, d, jnp.logical_and(jnp.logical_and(z < Z - 1, z > d), jnp.logical_not(low)))

    def sum_far(qs):
        for d in range(Z - 1, 0, -1):
            for q in qs:
                sum_step(q, 0, d, jnp.logical_and(z < d, jnp.logical_not(low)))
        for d in range(Z - 1):
            for q in qs:
                sum_step(q, 1, d, jnp.logical_and(z > d, low))

    def sum_end(q):
        j, i, h = units[q]
        for direction, there in ((0, z > 0), (1, z < Z - 1)):
            @pl.when(there)
            def _():
                sum_wait(q, direction, z)
                part[q, z] = part[q, z] + rs_r[q, direction, z].astype(F32)

        out[:, pl.ds(pl.multiple_of((fs_at(j, i) * cuts + h) * N, N), N)] = part[q, z].astype(BF16)

    in_row = [(0, i) for i in range(1, X)]
    in_col = [(j, 0) for j in range(1, Y)]
    both = range(cuts)
    early = [(j, i, 0) for j, i in in_row] + [(j, i, 1) for j, i in in_col] if cuts == 2 else []
    mid = [(j, i, h) for h in both for j, i in in_row + in_col if (j, i, h) not in early]
    qa = [q for h in both for q in down([(0, 0, h)])]
    phase_relay((2,))
    qb = down(early)
    sum_near(qa)
    wait_cross((2,))
    qc = down(mid)
    sum_near(qb)
    sum_far(qa)
    wait_diag((2,))
    qd = down([(j, i, h) for j, i in far for h in both])
    sum_near(qc)
    sum_far(qb)
    for q in qa + qb:
        sum_end(q)
    sum_far(qc)
    sum_near(qd)
    for q in qc:
        sum_end(q)
    sum_far(qd)
    for q in qd:
        sum_end(q)

    def sent(ref, sem):
        pltpu.make_async_copy(ref, ref, sem).wait()

    if F > 1:
        for m in range(3):
            sent(mats[m][1].at[pl.ds(0, F - 1)], w_send.at[m])
    for s in range(Z - 1):
        for direction in range(2):
            cp, ok = tok_chain(direction, s)
            pl.when(ok)(cp.wait_send)
    if C > 1:
        sent(nrm.at[c], ts_send)
        sent(sib_s, p_send)
    if Z > 1:
        sent(rs_s.at[:, pl.ds(0, Z - 1)], q_send)


def local(sizes, tokens, norm_gain, gate_weight, up_weight, down_weight):
    Y, X, Z, C = sizes
    F = Y * X
    rows, D = tokens.shape
    gate_weight, up_weight = gate_weight.T, up_weight.T
    H, K = gate_weight.shape
    cuts = 2 if down_weight.shape[1] % 256 == 0 else 1
    N = down_weight.shape[1] // cuts
    U = F * cuts
    tile = 2 if Z % 2 == 0 else 1
    vmem = pl.BlockSpec(memory_space=pltpu.VMEM)
    dma = pltpu.SemaphoreType.DMA
    hbm = pl.BlockSpec(memory_space=pl.ANY)
    return pl.pallas_call(
        functools.partial(kernel, Y, X, Z, C, cuts),
        out_shape=pltpu.VMEM((rows, D), BF16),
        in_specs=[hbm] * 5,
        out_specs=vmem,
        scratch_shapes=[
            pltpu.VMEM((C, Z, rows, D), BF16),
            pltpu.VMEM((F, H, K), BF16),
            pltpu.VMEM((F, H, K), BF16),
            pltpu.VMEM((F, H, N * cuts), BF16),
            pltpu.VMEM((C * Z // tile, tile * rows, H), F32),
            pltpu.VMEM((C * Z // tile, tile * rows, H), F32),
            pltpu.VMEM((C, Z, rows, H), BF16),
            pltpu.VMEM((U, Z, rows, N), BF16),
            pltpu.VMEM((U, Z, rows, N), BF16),
            pltpu.VMEM((U, Z, rows, N), BF16),
            pltpu.VMEM((U, 2, Z, rows, N), BF16),
            pltpu.VMEM((U, Z, rows, N), F32),
            pltpu.VMEM((rows, D), BF16),
            pltpu.VMEM((1, D), F32),
            dma((5,)),
            dma((3,)), dma((3, 2, F)),
            dma((2, max(Z - 1, 1))), dma((2, max(Z - 1, 1))), dma, dma((Z,)),
            dma, dma((U,)), dma, dma((U, Z + 1)),
        ],
        compiler_params=pltpu.CompilerParams(
            collective_id=0, has_side_effects=True, vmem_limit_bytes=60 * 1024 * 1024),
    )(tokens, norm_gain.reshape(1, D), gate_weight, up_weight, down_weight)


def solution(mesh):
    fs, tp = mesh.shape["fs"], mesh.shape["tp"]
    X = max(n for n in range(1, math.isqrt(fs) + 1) if fs % n == 0)
    C = 2 if tp % 2 == 0 else 1
    from jax.sharding import PartitionSpec as P
    return jax.shard_map(
        functools.partial(local, (fs // X, X, tp // C, C)),
        mesh=mesh,
        in_specs=(P(("fs", "tp"), None), P(), P("fs", "tp"), P("fs", "tp"), P("tp", "fs")),
        out_specs=P(("fs", "tp"), None),
        check_vma=False,
    )
```

```python
import functools
import math

import jax
import jax.numpy as jnp
from jax import lax
from jax.experimental import pallas as pl
from jax.experimental.pallas import tpu as pltpu

eps_floor = 0.05
MESH = pl.DeviceIdType.MESH
F32 = jnp.float32
BF16 = jnp.bfloat16


def kernel(Y, X, Z, C, cuts, tok, gain, gw, uw, dw, out, nrm, Wg, Wu, Wd, acc_g, acc_u, hid,
           sib_s, sib_r, rs_s, rs_r, part, tok_v, gain_v, w_local,
           w_send, w_recv, t_send, t_recv, ts_send, ts_recv, p_send, p_recv, q_send, q_recv):
    F = Y * X
    f = lax.axis_index("fs")
    t = lax.axis_index("tp")
    y, x = f // X, f % X
    z, c = t // C, t % C
    rows, D = tok.shape
    H, K = gw.shape
    N = dw.shape[1] // cuts
    tile = 2 if Z % 2 == 0 else 1

    def fs_at(j, i):
        return lax.rem(y + j, Y) * X + lax.rem(x + i, X)

    def tp_at(zz, cc):
        return zz * C + cc

    sib = lax.rem(c + 1, C)

    barrier = pltpu.get_barrier_semaphore()
    peers = [{"fs": fs_at(0, i)} for i in range(1, X)] + [{"fs": fs_at(j, 0)} for j in range(1, Y)]
    if C > 1:
        peers += [{"tp": tp_at(z, sib)}]

    def greet(peer):
        pl.semaphore_signal(barrier, inc=1, device_id=peer, device_id_type=MESH)

    for peer in peers:
        greet(peer)
    below, above = jnp.maximum(z - 1, 0), jnp.minimum(z + 1, Z - 1)
    pl.when(z > 0)(lambda: greet({"tp": tp_at(below, c)}))
    pl.when(z < Z - 1)(lambda: greet({"tp": tp_at(above, c)}))

    mats = ((gw, Wg), (uw, Wu), (dw, Wd))
    own_copies = [pltpu.make_async_copy(ref, held.at[f], w_local.at[m]) for m, (ref, held) in enumerate(mats)]
    own_copies += [pltpu.make_async_copy(tok, tok_v, w_local.at[3]), pltpu.make_async_copy(gain, gain_v, w_local.at[4])]
    for cp in own_copies:
        cp.start()

    pl.semaphore_wait(barrier, len(peers) + (z > 0).astype(jnp.int32) + (z < Z - 1).astype(jnp.int32))
    for cp in own_copies:
        cp.wait()

    def piece(m, h, j, i):
        held = mats[m][1].at[fs_at(j, i)]
        if m == 2 and cuts == 2:
            return held.at[:, pl.ds(h * N, N)]
        n = held.shape[0] // 2
        return held.at[pl.ds(h * n, n)]

    def w_copy(m, h, j, i, dj, di):
        slot = ((j - dj) % Y) * X + (i - di) % X
        cp = pltpu.make_async_remote_copy(
            src_ref=piece(m, h, j, i), dst_ref=piece(m, h, j, i),
            send_sem=w_send.at[m], recv_sem=w_recv.at[m, h, slot],
            device_id={"fs": fs_at(dj, di)}, device_id_type=MESH)
        cp.start()

    def w_wait(m, h, j, i):
        ref = piece(m, h, j, i)
        pltpu.make_async_copy(ref, ref, w_recv.at[m, h, j * X + i]).wait()

    def phase_one(ms):
        for m in ms:
            for i in range(1, X):
                w_copy(m, 0, 0, 0, 0, i)
            for j in range(1, Y):
                w_copy(m, 1, 0, 0, j, 0)

    def phase_own(ms):
        for m in ms:
            for i in range(1, X):
                w_copy(m, 1, 0, 0, 0, i)
            for j in range(1, Y):
                w_copy(m, 0, 0, 0, j, 0)

    def phase_relay(ms):
        for m in ms:
            for i in range(1, X):
                w_wait(m, 0, 0, i)
                for j in range(1, Y):
                    w_copy(m, 0, 0, i, j, 0)
            for j in range(1, Y):
                w_wait(m, 1, j, 0)
                for i in range(1, X):
                    w_copy(m, 1, j, 0, 0, i)

    def wait_cross(ms):
        for m in ms:
            for i in range(1, X):
                w_wait(m, 1, 0, i)
            for j in range(1, Y):
                w_wait(m, 0, j, 0)

    def wait_diag(ms):
        for m in ms:
            for j in range(1, Y):
                for i in range(1, X):
                    w_wait(m, 0, j, i)
                    w_wait(m, 1, j, i)

    def tok_chain(direction, s):
        src = z - s if direction == 0 else z + s
        dst = z + 1 if direction == 0 else z - 1
        ok = jnp.logical_and(src >= 0, dst < Z) if direction == 0 else jnp.logical_and(src < Z, dst >= 0)
        src, dst = jnp.clip(src, 0, Z - 1), jnp.clip(dst, 0, Z - 1)
        cp = pltpu.make_async_remote_copy(
            src_ref=nrm.at[c, src], dst_ref=nrm.at[c, src],
            send_sem=t_send.at[direction, s], recv_sem=t_recv.at[direction, s],
            device_id={"tp": tp_at(dst, c)}, device_id_type=MESH)
        return cp, ok

    def tok_sib(zz):
        return pltpu.make_async_remote_copy(
            src_ref=nrm.at[c, zz], dst_ref=nrm.at[c, zz],
            send_sem=ts_send, recv_sem=ts_recv.at[zz],
            device_id={"tp": tp_at(z, sib)}, device_id_type=MESH)

    def tok_start(s):
        for direction in range(2):
            cp, ok = tok_chain(direction, s)
            pl.when(ok)(cp.start)

    def tok_arrive(s):
        for direction in range(2):
            src = z - s if direction == 0 else z + s
            there = src >= 0 if direction == 0 else src < Z
            src = jnp.clip(src, 0, Z - 1)

            @pl.when(there)
            def _():
                pltpu.make_async_copy(nrm.at[c, src], nrm.at[c, src], t_recv.at[direction, s - 1]).wait()
                if C > 1:
                    tok_sib(src).start()

            if s < Z - 1:
                cp, ok = tok_chain(direction, s)
                pl.when(ok)(cp.start)

    phase_one((0, 1))
    values = tok_v[...].astype(F32)
    factor = lax.rsqrt(jnp.mean(values * values, axis=-1, keepdims=True) + eps_floor)
    nrm[c, z] = (values * factor * gain_v[...]).astype(BF16)
    tok_start(0)
    if C > 1:
        tok_sib(z).start()
    phase_own((0, 1))
    if Z > 1:
        tok_arrive(1)
    phase_relay((0, 1))
    for s in range(2, Z):
        tok_arrive(s)
    wait_cross((0, 1))
    phase_one((2,))
    phase_own((2,))
    if C > 1:
        for zz in range(Z):
            ref = nrm.at[sib, zz]
            pltpu.make_async_copy(ref, ref, ts_recv.at[zz]).wait()

    near = [(0, 0)] + [(0, i) for i in range(1, X)] + [(j, 0) for j in range(1, Y)]
    far = [(j, i) for j in range(1, Y) for i in range(1, X)]
    mrows = tile * rows
    per_core = Z // tile

    def product(n, held, group):
        cc, zt = n // per_core, n % per_core
        total = None
        for j, i in group:
            o = fs_at(j, i)
            a = nrm[cc, pl.ds(zt * tile, tile), :, pl.ds(pl.multiple_of(o * K, K), K)].reshape(mrows, K)
            p = lax.dot_general(a, held[o], (((1,), (1,)), ((), ())), preferred_element_type=F32)
            total = p if total is None else total + p
        return total

    @pl.loop(0, C * per_core)
    def _(n):
        acc_g[n] = product(n, Wg, near)
        acc_u[n] = product(n, Wu, near)

    wait_diag((0,))

    @pl.loop(0, C * per_core)
    def _(n):
        g = acc_g[n]
        if far:
            g = g + product(n, Wg, far)
        acc_g[n] = jax.nn.silu(g)

    wait_diag((1,))

    @pl.loop(0, C * per_core)
    def _(n):
        u = acc_u[n]
        if far:
            u = u + product(n, Wu, far)
        hid[n // per_core, pl.ds((n % per_core) * tile, tile)] = (acc_g[n] * u).astype(BF16).reshape(tile, rows, H)

    def sum_slot(direction, d, at):
        return d if direction == 0 else jnp.where(at == d, Z, d)

    def sum_copy(q, direction, d):
        to = above if direction == 0 else below
        return pltpu.make_async_remote_copy(
            src_ref=rs_s.at[q, d], dst_ref=rs_r.at[q, direction, d],
            send_sem=q_send, recv_sem=q_recv.at[q, sum_slot(direction, d, to)],
            device_id={"tp": tp_at(to, c)}, device_id_type=MESH)

    def sum_wait(q, direction, d):
        ref = rs_r.at[q, direction, d]
        pltpu.make_async_copy(ref, ref, q_recv.at[q, sum_slot(direction, d, z)]).wait()

    units = []

    def add_sib(q, d):
        if C > 1:
            part[q, d] = part[q, d] + sib_r[q, d].astype(F32)

    def open_sum(qs, direction, order):
        for d in order:
            for q in qs:
                total = part[q, d]
                if C > 1:
                    total = total + sib_r[q, d].astype(F32)
                rs_s[q, d] = total.astype(BF16)
                sum_copy(q, direction, d).start()

    def settle(qs, hold, held):
        def ends(direction, order):
            open_sum(qs, direction, order[:-1])
            if not hold:
                open_sum(held + qs, direction, order[-1:])

        if Z > 1:
            pl.when(z == 0)(lambda: ends(0, list(range(Z - 1, 0, -1))))
            pl.when(z == Z - 1)(lambda: ends(1, list(range(Z - 1))))

        @pl.loop(0, Z)
        def _(d):
            @pl.when(jnp.logical_or(d == z, jnp.logical_and(z > 0, z < Z - 1)))
            def _():
                for q in qs:
                    add_sib(q, d)

    def down(new, apart=False, hold=False, held=()):
        qs = list(range(len(units), len(units) + len(new)))
        units.extend(new)

        def weight(q):
            j, i, h = units[q]
            return Wd[fs_at(j, i), :, h * N:(h + 1) * N]

        copies = []
        if C > 1:
            for q in qs:
                sib_s[q] = jnp.dot(hid[sib].reshape(Z * rows, H), weight(q),
                                   preferred_element_type=F32).astype(BF16).reshape(Z, rows, N)
                cp = pltpu.make_async_remote_copy(
                    src_ref=sib_s.at[q], dst_ref=sib_r.at[q], send_sem=p_send, recv_sem=p_recv.at[q],
                    device_id={"tp": tp_at(z, sib)}, device_id_type=MESH)
                cp.start()
                copies.append(cp)
        for k, q in enumerate(qs):
            part[q] = jnp.dot(hid[c].reshape(Z * rows, H), weight(q),
                              preferred_element_type=F32).reshape(Z, rows, N)
            if C > 1:
                copies[k].wait_recv()
            if apart:
                settle([q], hold, [])
        if not apart:
            settle(qs, hold, list(held))
        return qs

    low = 2 * z < Z

    def sum_step(q, direction, d, ok):
        @pl.when(ok)
        def _():
            sum_wait(q, direction, d)
            rs_s[q, d] = (part[q, d] + rs_r[q, direction, d].astype(F32)).astype(BF16)
            sum_copy(q, direction, d).start()

    def near_low(q, k):
        d = Z - 1 - k
        sum_step(q, 0, d, jnp.logical_and(jnp.logical_and(z > 0, z < d), low))

    def near_high(q, k):
        sum_step(q, 1, k, jnp.logical_and(jnp.logical_and(z < Z - 1, z > k), jnp.logical_not(low)))

    def far_low(q, k):
        sum_step(q, 1, k, jnp.logical_and(z > k, low))

    def far_high(q, k):
        d = Z - 1 - k
        sum_step(q, 0, d, jnp.logical_and(z < d, jnp.logical_not(low)))

    hops = range(Z - 1)

    def sum_near(qs, ks=hops):
        for k in ks:
            for q in qs:
                near_low(q, k)
                near_high(q, k)

    def sum_far(qs):
        for k in hops:
            for q in qs:
                far_low(q, k)
                far_high(q, k)

    def sum_last(qs):
        for k in hops:
            for q in qs:
                if k + 1 < Z - 1:
                    near_low(q, k + 1)
                far_low(q, k)
                far_high(q, k)
                if k + 1 < Z - 1:
                    near_high(q, k + 1)

    def sum_end(q):
        j, i, h = units[q]
        for direction, there in ((0, z > 0), (1, z < Z - 1)):
            @pl.when(there)
            def _():
                sum_wait(q, direction, z)
                part[q, z] = part[q, z] + rs_r[q, direction, z].astype(F32)

        out[:, pl.ds(pl.multiple_of((fs_at(j, i) * cuts + h) * N, N), N)] = part[q, z].astype(BF16)

    in_row = [(0, i) for i in range(1, X)]
    in_col = [(j, 0) for j in range(1, Y)]
    both = range(cuts)
    early = [(j, i, 0) for j, i in in_row] + [(j, i, 1) for j, i in in_col] if cuts == 2 else []
    mid = [(j, i, h) for h in both for j, i in in_row + in_col if (j, i, h) not in early]
    qa = down([(0, 0, h) for h in both], True)
    phase_relay((2,))
    qb = down(early)
    sum_near(qa)
    wait_cross((2,))
    qc = down(mid, hold=True)
    sum_near(qb)
    sum_far(qa)
    wait_diag((2,))
    qd = down([(j, i, h) for j, i in far for h in both], held=qc)
    sum_near(qc)
    sum_far(qb)
    for q in qa + qb:
        sum_end(q)
    sum_far(qc)
    sum_near(qd, range(min(1, Z - 1)))
    sum_last(qd)
    for q in qc + qd:
        sum_end(q)

    def sent(ref, sem):
        pltpu.make_async_copy(ref, ref, sem).wait()

    if F > 1:
        for m in range(3):
            sent(mats[m][1].at[pl.ds(0, F - 1)], w_send.at[m])
    for s in range(Z - 1):
        for direction in range(2):
            cp, ok = tok_chain(direction, s)
            pl.when(ok)(cp.wait_send)
    if C > 1:
        sent(nrm.at[c], ts_send)
        sent(sib_s, p_send)
    if Z > 1:
        sent(rs_s.at[:, pl.ds(0, Z - 1)], q_send)


def local(sizes, tokens, norm_gain, gate_weight, up_weight, down_weight):
    Y, X, Z, C = sizes
    F = Y * X
    rows, D = tokens.shape
    gate_weight, up_weight = gate_weight.T, up_weight.T
    H, K = gate_weight.shape
    cuts = 2 if down_weight.shape[1] % 256 == 0 else 1
    N = down_weight.shape[1] // cuts
    U = F * cuts
    tile = 2 if Z % 2 == 0 else 1
    vmem = pl.BlockSpec(memory_space=pltpu.VMEM)
    dma = pltpu.SemaphoreType.DMA
    hbm = pl.BlockSpec(memory_space=pl.ANY)
    return pl.pallas_call(
        functools.partial(kernel, Y, X, Z, C, cuts),
        out_shape=pltpu.VMEM((rows, D), BF16),
        in_specs=[hbm] * 5,
        out_specs=vmem,
        scratch_shapes=[
            pltpu.VMEM((C, Z, rows, D), BF16),
            pltpu.VMEM((F, H, K), BF16),
            pltpu.VMEM((F, H, K), BF16),
            pltpu.VMEM((F, H, N * cuts), BF16),
            pltpu.VMEM((C * Z // tile, tile * rows, H), F32),
            pltpu.VMEM((C * Z // tile, tile * rows, H), F32),
            pltpu.VMEM((C, Z, rows, H), BF16),
            pltpu.VMEM((U, Z, rows, N), BF16),
            pltpu.VMEM((U, Z, rows, N), BF16),
            pltpu.VMEM((U, Z, rows, N), BF16),
            pltpu.VMEM((U, 2, Z, rows, N), BF16),
            pltpu.VMEM((U, Z, rows, N), F32),
            pltpu.VMEM((rows, D), BF16),
            pltpu.VMEM((1, D), F32),
            dma((5,)),
            dma((3,)), dma((3, 2, F)),
            dma((2, max(Z - 1, 1))), dma((2, max(Z - 1, 1))), dma, dma((Z,)),
            dma, dma((U,)), dma, dma((U, Z + 1)),
        ],
        compiler_params=pltpu.CompilerParams(
            collective_id=0, has_side_effects=True, vmem_limit_bytes=60 * 1024 * 1024),
    )(tokens, norm_gain.reshape(1, D), gate_weight, up_weight, down_weight)


def solution(mesh):
    fs, tp = mesh.shape["fs"], mesh.shape["tp"]
    X = max(n for n in range(1, math.isqrt(fs) + 1) if fs % n == 0)
    C = 2 if tp % 2 == 0 else 1
    from jax.sharding import PartitionSpec as P
    return jax.shard_map(
        functools.partial(local, (fs // X, X, tp // C, C)),
        mesh=mesh,
        in_specs=(P(("fs", "tp"), None), P(), P("fs", "tp"), P("fs", "tp"), P("tp", "fs")),
        out_specs=P(("fs", "tp"), None),
        check_vma=False,
    )
```

```python
import functools
import math

import jax
import jax.numpy as jnp
from jax import lax
from jax.experimental import pallas as pl
from jax.experimental.pallas import tpu as pltpu

eps_floor = 0.05
MESH = pl.DeviceIdType.MESH
F32 = jnp.float32
BF16 = jnp.bfloat16


def kernel(Y, X, Z, C, cuts, R, tok, gain, gw, uw, dw, out, nrm, Wg, Wu, Wd, over, acc_g, acc_u, hid,
           sib_s, sib_r, rs_s, rs_r, part, tok_v, gain_v, w_local,
           w_send, w_recv, over_recv, t_send, t_recv, ts_send, ts_recv, p_send, p_recv, q_send, q_recv):
    F = Y * X
    f = lax.axis_index("fs")
    t = lax.axis_index("tp")
    y, x = f // X, f % X
    z, c = t // C, t % C
    rows, D = tok.shape
    H, K = gw.shape
    N = dw.shape[1] // cuts
    tile = 2 if Z % 2 == 0 else 1
    n0 = H // 2 - R
    strips = 2 if rows % 32 == 0 else 1
    strip = rows // strips
    ups = (1, 3) if R else (1,)
    edge = jnp.logical_or(z == 0, z == Z - 1)
    inner = jnp.logical_or(z == 1, z == Z - 2)

    def fs_at(j, i):
        return lax.rem(y + j, Y) * X + lax.rem(x + i, X)

    def tp_at(zz, cc):
        return zz * C + cc

    sib = lax.rem(c + 1, C)

    barrier = pltpu.get_barrier_semaphore()
    peers = [{"fs": fs_at(0, i)} for i in range(1, X)] + [{"fs": fs_at(j, 0)} for j in range(1, Y)]
    if C > 1:
        peers += [{"tp": tp_at(z, sib)}]

    def greet(peer):
        pl.semaphore_signal(barrier, inc=1, device_id=peer, device_id_type=MESH)

    for peer in peers:
        greet(peer)
    below, above = jnp.maximum(z - 1, 0), jnp.minimum(z + 1, Z - 1)
    pl.when(z > 0)(lambda: greet({"tp": tp_at(below, c)}))
    pl.when(z < Z - 1)(lambda: greet({"tp": tp_at(above, c)}))

    mats = ((gw, Wg), (uw, Wu), (dw, Wd))
    own_copies = [pltpu.make_async_copy(ref, held.at[f], w_local.at[m]) for m, (ref, held) in enumerate(mats)]
    own_copies += [pltpu.make_async_copy(tok, tok_v, w_local.at[3]), pltpu.make_async_copy(gain, gain_v, w_local.at[4])]
    for cp in own_copies:
        cp.start()

    pl.semaphore_wait(barrier, len(peers) + (z > 0).astype(jnp.int32) + (z < Z - 1).astype(jnp.int32))
    for cp in own_copies:
        cp.wait()

    def piece(m, h, j, i):
        o = fs_at(j, i)
        if m == 0:
            return Wg.at[o, pl.ds(h * (H // 2), H // 2)]
        if m == 1:
            return Wu.at[o, pl.ds(h * n0, n0)]
        if m == 3:
            return Wu.at[o, pl.ds(2 * n0 + h * R, R)]
        if m == 4:
            return over.at[o, pl.ds(h * R, R)]
        if cuts == 2:
            return Wd.at[o, :, pl.ds(h * N, N)]
        return Wd.at[o, pl.ds(h * (H // 2), H // 2)]

    def w_copy(m, h, j, i, dj, di):
        slot = ((j - dj) % Y) * X + (i - di) % X
        cp = pltpu.make_async_remote_copy(
            src_ref=piece(m, h, j, i), dst_ref=piece(m, h, j, i),
            send_sem=w_send.at[m], recv_sem=w_recv.at[m, h, slot - 1],
            device_id={"fs": fs_at(dj, di)}, device_id_type=MESH)
        cp.start()

    def w_wait(m, h, j, i):
        ref = piece(m, h, j, i)
        pltpu.make_async_copy(ref, ref, w_recv.at[m, h, j * X + i - 1]).wait()

    def phase_one(ms):
        for m in ms:
            for i in range(1, X):
                w_copy(m, 0, 0, 0, 0, i)
            for j in range(1, Y):
                w_copy(m, 1, 0, 0, j, 0)

    def phase_own(ms):
        for m in ms:
            for i in range(1, X):
                w_copy(m, 1, 0, 0, 0, i)
            for j in range(1, Y):
                w_copy(m, 0, 0, 0, j, 0)

    def phase_relay(ms):
        for m in ms:
            for i in range(1, X):
                w_wait(m, 0, 0, i)
                for j in range(1, Y):
                    w_copy(m, 0, 0, i, j, 0)
            for j in range(1, Y):
                w_wait(m, 1, j, 0)
                for i in range(1, X):
                    w_copy(m, 1, j, 0, 0, i)

    def wait_cross(ms):
        for m in ms:
            for i in range(1, X):
                w_wait(m, 1, 0, i)
            for j in range(1, Y):
                w_wait(m, 0, j, 0)

    def wait_diag(ms):
        for m in ms:
            for j in range(1, Y):
                for i in range(1, X):
                    w_wait(m, 0, j, i)
                    w_wait(m, 1, j, i)

    def over_in():
        o = fs_at(0, 0)
        to = jnp.where(z == 0, 1, Z - 2)
        return pltpu.make_async_remote_copy(
            src_ref=Wu.at[o, pl.ds(2 * n0, 2 * R)], dst_ref=over.at[o],
            send_sem=w_send.at[3], recv_sem=over_recv,
            device_id={"tp": tp_at(to, c)}, device_id_type=MESH)

    def over_out(group):
        to = jnp.where(z == 1, 0, Z - 1)
        for j, i in group:
            for h in range(2):
                pltpu.make_async_remote_copy(
                    src_ref=piece(4, h, j, i), dst_ref=piece(3, h, j, i),
                    send_sem=w_send.at[5], recv_sem=w_recv.at[3, h, j * X + i - 1],
                    device_id={"tp": tp_at(to, c)}, device_id_type=MESH).start()

    def tok_chain(direction, s, a):
        src = z - s if direction == 0 else z + s
        dst = z + 1 if direction == 0 else z - 1
        ok = jnp.logical_and(src >= 0, dst < Z) if direction == 0 else jnp.logical_and(src < Z, dst >= 0)
        src, dst = jnp.clip(src, 0, Z - 1), jnp.clip(dst, 0, Z - 1)
        ref = nrm.at[c, src, pl.ds(a * strip, strip)]
        cp = pltpu.make_async_remote_copy(
            src_ref=ref, dst_ref=ref,
            send_sem=t_send.at[direction], recv_sem=t_recv.at[direction, s, a],
            device_id={"tp": tp_at(dst, c)}, device_id_type=MESH)
        return cp, ok

    def tok_sib(zz, a):
        ref = nrm.at[c, zz, pl.ds(a * strip, strip)]
        return pltpu.make_async_remote_copy(
            src_ref=ref, dst_ref=ref,
            send_sem=ts_send, recv_sem=ts_recv,
            device_id={"tp": tp_at(z, sib)}, device_id_type=MESH)

    def tok_arrive(s, a):
        for direction in range(2):
            src = z - s if direction == 0 else z + s
            there = src >= 0 if direction == 0 else src < Z
            src = jnp.clip(src, 0, Z - 1)

            @pl.when(there)
            def _():
                ref = nrm.at[c, src, pl.ds(a * strip, strip)]
                pltpu.make_async_copy(ref, ref, t_recv.at[direction, s - 1, a]).wait()
                if C > 1:
                    tok_sib(src, a).start()

            if s < Z - 1:
                cp, ok = tok_chain(direction, s, a)
                pl.when(ok)(cp.start)

    def over_relay():
        for i in range(1, X):
            w_wait(4, 0, 0, i)
            for j in range(1, Y):
                w_copy(4, 0, 0, i, j, 0)
        for j in range(1, Y):
            w_wait(4, 1, j, 0)
            for i in range(1, X):
                w_copy(4, 1, j, 0, 0, i)

    def edge_direct():
        for i in range(1, X):
            w_wait(3, 0, 0, i)
        for j in range(1, Y):
            w_wait(3, 1, j, 0)

    def over_cross():
        wait_cross((4,))
        over_out(in_row + in_col)

    def over_diag():
        wait_diag((4,))
        over_out(far)

    in_row = [(0, i) for i in range(1, X)]
    in_col = [(j, 0) for j in range(1, Y)]
    far = [(j, i) for j in range(1, Y) for i in range(1, X)]

    phase_one((0, 1))
    if R:
        pl.when(edge)(lambda: over_in().start())
    for a in range(strips):
        part_rows = pl.ds(a * strip, strip)
        values = tok_v[part_rows, :].astype(F32)
        factor = lax.rsqrt(jnp.mean(values * values, axis=-1, keepdims=True) + eps_floor)
        nrm[c, z, part_rows] = (values * factor * gain_v[...]).astype(BF16)
        for direction in range(2):
            cp, ok = tok_chain(direction, 0, a)
            pl.when(ok)(cp.start)
        if C > 1:
            tok_sib(z, a).start()
    if R:
        @pl.when(inner)
        def _():
            pltpu.make_async_copy(over.at[f], over.at[f], over_recv).wait()
            phase_one((4,))
            phase_own((4,))
    phase_own((0, 1))
    if R:
        @pl.when(jnp.logical_not(edge))
        def _():
            phase_one((3,))
            phase_own((3,))
    if Z > 1:
        for a in range(strips):
            tok_arrive(1, a)
    if Z > 2:
        tok_arrive(2, 0)
    if R:
        pl.when(inner)(over_relay)
    phase_relay((0, 1))
    if Z > 2:
        for a in range(1, strips):
            tok_arrive(2, a)
    if R:
        pl.when(inner)(over_cross)
        pl.when(jnp.logical_not(edge))(lambda: phase_relay((3,)))
    for s in range(3, Z):
        for a in range(strips):
            tok_arrive(s, a)
    phase_one((2,))
    phase_own((2,))
    if R:
        pl.when(inner)(over_diag)
    if C > 1:
        pltpu.make_async_copy(nrm.at[sib], nrm.at[sib], ts_recv).wait()

    near = [(0, 0)] + [(0, i) for i in range(1, X)] + [(j, 0) for j in range(1, Y)]
    mrows = tile * rows
    per_core = Z // tile

    def product(n, held, group):
        cc, zt = n // per_core, n % per_core
        total = None
        for j, i in group:
            o = fs_at(j, i)
            a = nrm[cc, pl.ds(zt * tile, tile), :, pl.ds(pl.multiple_of(o * K, K), K)].reshape(mrows, K)
            p = lax.dot_general(a, held[o], (((1,), (1,)), ((), ())), preferred_element_type=F32)
            total = p if total is None else total + p
        return total

    wait_cross((0,))

    @pl.loop(0, C * per_core)
    def _(n):
        acc_g[n] = product(n, Wg, near)

    wait_diag((0,))

    @pl.loop(0, C * per_core)
    def _(n):
        g = acc_g[n]
        if far:
            g = g + product(n, Wg, far)
        acc_g[n] = jax.nn.silu(g)

    if R:
        pl.when(edge)(edge_direct)
    wait_cross(ups)

    @pl.loop(0, C * per_core)
    def _(n):
        acc_u[n] = product(n, Wu, near)

    wait_diag(ups)

    @pl.loop(0, C * per_core)
    def _(n):
        u = acc_u[n]
        if far:
            u = u + product(n, Wu, far)
        hid[n // per_core, pl.ds((n % per_core) * tile, tile)] = (acc_g[n] * u).astype(BF16).reshape(tile, rows, H)

    def sum_slot(direction, d, at):
        return d if direction == 0 else jnp.where(at == d, Z, d)

    def sum_copy(q, direction, d):
        to = above if direction == 0 else below
        return pltpu.make_async_remote_copy(
            src_ref=rs_s.at[q, d], dst_ref=rs_r.at[q, direction, d],
            send_sem=q_send, recv_sem=q_recv.at[q, sum_slot(direction, d, to)],
            device_id={"tp": tp_at(to, c)}, device_id_type=MESH)

    def sum_wait(q, direction, d):
        ref = rs_r.at[q, direction, d]
        pltpu.make_async_copy(ref, ref, q_recv.at[q, sum_slot(direction, d, z)]).wait()

    units = []

    def add_sib(q, d):
        if C > 1:
            part[q, d] = part[q, d] + sib_r[q, d].astype(F32)

    def open_sum(qs, direction, order):
        for d in order:
            for q in qs:
                total = part[q, d]
                if C > 1:
                    total = total + sib_r[q, d].astype(F32)
                rs_s[q, d] = total.astype(BF16)
                sum_copy(q, direction, d).start()

    def settle(qs, hold, held):
        def ends(direction, order):
            open_sum(qs, direction, order[:-1])
            if not hold:
                open_sum(held + qs, direction, order[-1:])

        if Z > 1:
            pl.when(z == 0)(lambda: ends(0, list(range(Z - 1, 0, -1))))
            pl.when(z == Z - 1)(lambda: ends(1, list(range(Z - 1))))

        @pl.loop(0, Z)
        def _(d):
            @pl.when(jnp.logical_or(d == z, jnp.logical_and(z > 0, z < Z - 1)))
            def _():
                for q in qs:
                    add_sib(q, d)

    def down(new, apart=False, hold=False, held=()):
        qs = list(range(len(units), len(units) + len(new)))
        units.extend(new)

        def weight(q):
            j, i, h = units[q]
            return Wd[fs_at(j, i), :, h * N:(h + 1) * N]

        copies = []
        if C > 1:
            for q in qs:
                sib_s[q] = jnp.dot(hid[sib].reshape(Z * rows, H), weight(q),
                                   preferred_element_type=F32).astype(BF16).reshape(Z, rows, N)
                cp = pltpu.make_async_remote_copy(
                    src_ref=sib_s.at[q], dst_ref=sib_r.at[q], send_sem=p_send, recv_sem=p_recv.at[q],
                    device_id={"tp": tp_at(z, sib)}, device_id_type=MESH)
                cp.start()
                copies.append(cp)
        for k, q in enumerate(qs):
            part[q] = jnp.dot(hid[c].reshape(Z * rows, H), weight(q),
                              preferred_element_type=F32).reshape(Z, rows, N)
            if C > 1:
                copies[k].wait_recv()
            if apart:
                settle([q], hold, [])
        if not apart:
            settle(qs, hold, list(held))
        return qs

    low = 2 * z < Z

    def sum_step(q, direction, d, ok):
        @pl.when(ok)
        def _():
            sum_wait(q, direction, d)
            rs_s[q, d] = (part[q, d] + rs_r[q, direction, d].astype(F32)).astype(BF16)
            sum_copy(q, direction, d).start()

    def near_low(q, k):
        d = Z - 1 - k
        sum_step(q, 0, d, jnp.logical_and(jnp.logical_and(z > 0, z < d), low))

    def near_high(q, k):
        sum_step(q, 1, k, jnp.logical_and(jnp.logical_and(z < Z - 1, z > k), jnp.logical_not(low)))

    def far_low(q, k):
        sum_step(q, 1, k, jnp.logical_and(z > k, low))

    def far_high(q, k):
        d = Z - 1 - k
        sum_step(q, 0, d, jnp.logical_and(z < d, jnp.logical_not(low)))

    hops = range(Z - 1)

    def sum_near(qs, ks=hops):
        for k in ks:
            for q in qs:
                near_low(q, k)
                near_high(q, k)

    def sum_far(qs):
        for k in hops:
            for q in qs:
                far_low(q, k)
                far_high(q, k)

    def sum_end(q):
        j, i, h = units[q]
        for direction, there in ((0, z > 0), (1, z < Z - 1)):
            @pl.when(there)
            def _():
                sum_wait(q, direction, z)
                part[q, z] = part[q, z] + rs_r[q, direction, z].astype(F32)

        out[:, pl.ds(pl.multiple_of((fs_at(j, i) * cuts + h) * N, N), N)] = part[q, z].astype(BF16)

    both = range(cuts)
    early = [(j, i, 0) for j, i in in_row] + [(j, i, 1) for j, i in in_col] if cuts == 2 else []
    mid = [(j, i, h) for h in both for j, i in in_row + in_col if (j, i, h) not in early]
    qa = down([(0, 0, h) for h in both], True)
    sum_near(qa)
    phase_relay((2,))
    qb = down(early)
    sum_near(qb)
    sum_far(qa)
    wait_cross((2,))
    qc = down(mid, hold=True)
    sum_near(qc)
    sum_far(qb)
    wait_diag((2,))
    qd = down([(j, i, h) for j, i in far for h in both], held=qc)
    sum_near(qd)
    sum_far(qc)
    for q in qa + qb:
        sum_end(q)
    sum_far(qd)
    for q in qc + qd:
        sum_end(q)

    def sent(ref, sem):
        pltpu.make_async_copy(ref, ref, sem).wait()

    if F > 1:
        most = pl.ds(0, F - 1)
        sent(Wg.at[most], w_send.at[0])
        sent(Wu.at[most, pl.ds(0, 2 * n0)], w_send.at[1])
        sent(Wd.at[most], w_send.at[2])
        if R:
            pl.when(jnp.logical_not(edge))(lambda: sent(Wu.at[most, pl.ds(2 * n0, 2 * R)], w_send.at[3]))

            @pl.when(inner)
            def _():
                sent(over.at[most], w_send.at[4])
                sent(over.at[most], w_send.at[5])
    if R:
        pl.when(edge)(lambda: sent(over.at[f], w_send.at[3]))
    for k in range(Z):
        if k < Z - 1:
            pl.when(z == k)(lambda: sent(nrm.at[c, pl.ds(0, k + 1)], t_send.at[0]))
        if k > 0:
            pl.when(z == k)(lambda: sent(nrm.at[c, pl.ds(k, Z - k)], t_send.at[1]))
    if C > 1:
        sent(nrm.at[c], ts_send)
        sent(sib_s, p_send)
    if Z > 1:
        sent(rs_s.at[:, pl.ds(0, Z - 1)], q_send)


def local(sizes, tokens, norm_gain, gate_weight, up_weight, down_weight):
    Y, X, Z, C = sizes
    F = Y * X
    rows, D = tokens.shape
    gate_weight, up_weight = gate_weight.T, up_weight.T
    H, K = gate_weight.shape
    cuts = 2 if down_weight.shape[1] % 256 == 0 else 1
    N = down_weight.shape[1] // cuts
    U = F * cuts
    tile = 2 if Z % 2 == 0 else 1
    R = max(H * 3 // 44 // 16, 1) * 16 if Z >= 4 and F > 1 and H % 32 == 0 else 0
    strips = 2 if rows % 32 == 0 else 1
    vmem = pl.BlockSpec(memory_space=pltpu.VMEM)
    dma = pltpu.SemaphoreType.DMA
    hbm = pl.BlockSpec(memory_space=pl.ANY)
    return pl.pallas_call(
        functools.partial(kernel, Y, X, Z, C, cuts, R),
        out_shape=pltpu.VMEM((rows, D), BF16),
        in_specs=[hbm] * 5,
        out_specs=vmem,
        scratch_shapes=[
            pltpu.VMEM((C, Z, rows, D), BF16),
            pltpu.VMEM((F, H, K), BF16),
            pltpu.VMEM((F, H, K), BF16),
            pltpu.VMEM((F, H, N * cuts), BF16),
            pltpu.VMEM((F, 2 * max(R, 8), K), BF16),
            pltpu.VMEM((C * Z // tile, tile * rows, H), F32),
            pltpu.VMEM((C * Z // tile, tile * rows, H), F32),
            pltpu.VMEM((C, Z, rows, H), BF16),
            pltpu.VMEM((U, Z, rows, N), BF16),
            pltpu.VMEM((U, Z, rows, N), BF16),
            pltpu.VMEM((U, Z, rows, N), BF16),
            pltpu.VMEM((U, 2, Z, rows, N), BF16),
            pltpu.VMEM((U, Z, rows, N), F32),
            pltpu.VMEM((rows, D), BF16),
            pltpu.VMEM((1, D), F32),
            dma((5,)),
            dma((6,)), dma((5, 2, max(F - 1, 1))), dma,
            dma((2,)), dma((2, max(Z - 1, 1), strips)), dma, dma,
            dma, dma((U,)), dma, dma((U, Z + 1)),
        ],
        compiler_params=pltpu.CompilerParams(
            collective_id=0, has_side_effects=True, vmem_limit_bytes=60 * 1024 * 1024),
    )(tokens, norm_gain.reshape(1, D), gate_weight, up_weight, down_weight)


def solution(mesh):
    fs, tp = mesh.shape["fs"], mesh.shape["tp"]
    X = max(n for n in range(1, math.isqrt(fs) + 1) if fs % n == 0)
    C = 2 if tp % 2 == 0 else 1
    from jax.sharding import PartitionSpec as P
    return jax.shard_map(
        functools.partial(local, (fs // X, X, tp // C, C)),
        mesh=mesh,
        in_specs=(P(("fs", "tp"), None), P(), P("fs", "tp"), P("fs", "tp"), P("tp", "fs")),
        out_specs=P(("fs", "tp"), None),
        check_vma=False,
    )
```

```python
import functools
import math

import jax
import jax.numpy as jnp
from jax import lax
from jax.experimental import pallas as pl
from jax.experimental.pallas import tpu as pltpu

eps_floor = 0.05
MESH = pl.DeviceIdType.MESH
F32 = jnp.float32
BF16 = jnp.bfloat16


def kernel(Y, X, Z, C, cuts, R, tok, gain, gw, uw, dw, out, nrm, Wg, Wu, Wd, over, acc_g, acc_u, hid,
           sib_s, sib_r, rs_s, rs_r, part, tok_v, gain_v, w_local,
           w_send, w_recv, over_recv, t_send, t_recv, ts_send, ts_recv, p_send, p_recv, q_send, q_recv):
    F = Y * X
    f = lax.axis_index("fs")
    t = lax.axis_index("tp")
    y, x = f // X, f % X
    z, c = t // C, t % C
    rows, D = tok.shape
    H, K = gw.shape
    N = dw.shape[1] // cuts
    tile = 2 if Z % 2 == 0 else 1
    n0 = H // 2 - R
    strips = 2 if rows % 32 == 0 else 1
    strip = rows // strips
    ups = (1, 3) if R else (1,)
    halves = (5, 6)
    home = z // tile
    edge = jnp.logical_or(z == 0, z == Z - 1)
    inner = jnp.logical_or(z == 1, z == Z - 2)

    def fs_at(j, i):
        return lax.rem(y + j, Y) * X + lax.rem(x + i, X)

    def tp_at(zz, cc):
        return zz * C + cc

    sib = lax.rem(c + 1, C)

    barrier = pltpu.get_barrier_semaphore()
    peers = [{"fs": fs_at(0, i)} for i in range(1, X)] + [{"fs": fs_at(j, 0)} for j in range(1, Y)]
    if C > 1:
        peers += [{"tp": tp_at(z, sib)}]

    def greet(peer):
        pl.semaphore_signal(barrier, inc=1, device_id=peer, device_id_type=MESH)

    for peer in peers:
        greet(peer)
    below, above = jnp.maximum(z - 1, 0), jnp.minimum(z + 1, Z - 1)
    pl.when(z > 0)(lambda: greet({"tp": tp_at(below, c)}))
    pl.when(z < Z - 1)(lambda: greet({"tp": tp_at(above, c)}))

    mats = ((gw, Wg), (uw, Wu), (dw, Wd))
    own_copies = [pltpu.make_async_copy(ref, held.at[f], w_local.at[m]) for m, (ref, held) in enumerate(mats)]
    own_copies += [pltpu.make_async_copy(tok, tok_v, w_local.at[3]), pltpu.make_async_copy(gain, gain_v, w_local.at[4])]
    for cp in own_copies:
        cp.start()

    pl.semaphore_wait(barrier, len(peers) + (z > 0).astype(jnp.int32) + (z < Z - 1).astype(jnp.int32))
    for cp in own_copies:
        cp.wait()

    def piece(m, h, j, i):
        o = fs_at(j, i)
        if m == 0:
            return Wg.at[o, pl.ds(h * (H // 2), H // 2)]
        if m == 1:
            return Wu.at[o, pl.ds(h * n0, n0)]
        if m == 3:
            return Wu.at[o, pl.ds(2 * n0 + h * R, R)]
        if m == 4:
            return over.at[o, pl.ds(h * R, R)]
        if m in (5, 6):
            return Wd.at[o, pl.ds((m - 5) * (H // 2), H // 2), pl.ds(h * N, N)]
        return Wd.at[o, :, pl.ds(h * N, N)]

    def w_copy(m, h, j, i, dj, di):
        slot = ((j - dj) % Y) * X + (i - di) % X
        cp = pltpu.make_async_remote_copy(
            src_ref=piece(m, h, j, i), dst_ref=piece(m, h, j, i),
            send_sem=w_send.at[2 if m in halves else m], recv_sem=w_recv.at[m, h, slot - 1],
            device_id={"fs": fs_at(dj, di)}, device_id_type=MESH)
        cp.start()

    def w_wait(m, h, j, i):
        ref = piece(m, h, j, i)
        pltpu.make_async_copy(ref, ref, w_recv.at[m, h, j * X + i - 1]).wait()

    def phase_one(ms):
        for m in ms:
            for i in range(1, X):
                w_copy(m, 0, 0, 0, 0, i)
            for j in range(1, Y):
                w_copy(m, 1, 0, 0, j, 0)

    def phase_own(ms):
        for m in ms:
            for i in range(1, X):
                w_copy(m, 1, 0, 0, 0, i)
            for j in range(1, Y):
                w_copy(m, 0, 0, 0, j, 0)

    def phase_relay(ms):
        for m in ms:
            for i in range(1, X):
                w_wait(m, 0, 0, i)
                for j in range(1, Y):
                    w_copy(m, 0, 0, i, j, 0)
            for j in range(1, Y):
                w_wait(m, 1, j, 0)
                for i in range(1, X):
                    w_copy(m, 1, j, 0, 0, i)

    def down_send(h):
        for i in range(1, X):
            w_copy(2, h, 0, 0, 0, i)
        for j in range(1, Y):
            w_copy(2, h, 0, 0, j, 0)

    def down_relay(h):
        for i in range(1, X):
            w_wait(2, h, 0, i)
            for j in range(1, Y):
                w_copy(5, h, 0, i, j, 0)
        for j in range(1, Y):
            w_wait(2, h, j, 0)
            for i in range(1, X):
                w_copy(6, h, j, 0, 0, i)

    def down_diag(h):
        for j, i in far:
            w_wait(5, h, j, i)
            w_wait(6, h, j, i)

    def wait_cross(ms):
        for m in ms:
            for i in range(1, X):
                w_wait(m, 1, 0, i)
            for j in range(1, Y):
                w_wait(m, 0, j, 0)

    def wait_diag(ms):
        for m in ms:
            for j in range(1, Y):
                for i in range(1, X):
                    w_wait(m, 0, j, i)
                    w_wait(m, 1, j, i)

    def over_in():
        o = fs_at(0, 0)
        to = jnp.where(z == 0, 1, Z - 2)
        return pltpu.make_async_remote_copy(
            src_ref=Wu.at[o, pl.ds(2 * n0, 2 * R)], dst_ref=over.at[o],
            send_sem=w_send.at[3], recv_sem=over_recv,
            device_id={"tp": tp_at(to, c)}, device_id_type=MESH)

    def over_out(group):
        to = jnp.where(z == 1, 0, Z - 1)
        for j, i in group:
            for h in range(2):
                pltpu.make_async_remote_copy(
                    src_ref=piece(4, h, j, i), dst_ref=piece(3, h, j, i),
                    send_sem=w_send.at[5], recv_sem=w_recv.at[3, h, j * X + i - 1],
                    device_id={"tp": tp_at(to, c)}, device_id_type=MESH).start()

    def tok_chain(direction, s, a):
        src = z - s if direction == 0 else z + s
        dst = z + 1 if direction == 0 else z - 1
        ok = jnp.logical_and(src >= 0, dst < Z) if direction == 0 else jnp.logical_and(src < Z, dst >= 0)
        src, dst = jnp.clip(src, 0, Z - 1), jnp.clip(dst, 0, Z - 1)
        ref = nrm.at[c, src, pl.ds(a * strip, strip)]
        cp = pltpu.make_async_remote_copy(
            src_ref=ref, dst_ref=ref,
            send_sem=t_send.at[direction], recv_sem=t_recv.at[direction, s, a],
            device_id={"tp": tp_at(dst, c)}, device_id_type=MESH)
        return cp, ok

    def tok_sib(zz, a):
        ref = nrm.at[c, zz, pl.ds(a * strip, strip)]
        return pltpu.make_async_remote_copy(
            src_ref=ref, dst_ref=ref,
            send_sem=ts_send, recv_sem=ts_recv.at[jnp.where(zz // tile == home, 0, 1)],
            device_id={"tp": tp_at(z, sib)}, device_id_type=MESH)

    def tok_arrive(s, a):
        for direction in range(2):
            src = z - s if direction == 0 else z + s
            there = src >= 0 if direction == 0 else src < Z
            src = jnp.clip(src, 0, Z - 1)

            @pl.when(there)
            def _():
                ref = nrm.at[c, src, pl.ds(a * strip, strip)]
                pltpu.make_async_copy(ref, ref, t_recv.at[direction, s - 1, a]).wait()
                if C > 1:
                    tok_sib(src, a).start()

            if s < Z - 1:
                cp, ok = tok_chain(direction, s, a)
                pl.when(ok)(cp.start)

    def over_relay():
        for i in range(1, X):
            w_wait(4, 0, 0, i)
            for j in range(1, Y):
                w_copy(4, 0, 0, i, j, 0)
        for j in range(1, Y):
            w_wait(4, 1, j, 0)
            for i in range(1, X):
                w_copy(4, 1, j, 0, 0, i)

    def edge_direct():
        for i in range(1, X):
            w_wait(3, 0, 0, i)
        for j in range(1, Y):
            w_wait(3, 1, j, 0)

    def over_cross():
        wait_cross((4,))
        over_out(in_row + in_col)

    def over_diag():
        wait_diag((4,))
        over_out(far)

    in_row = [(0, i) for i in range(1, X)]
    in_col = [(j, 0) for j in range(1, Y)]
    far = [(j, i) for j in range(1, Y) for i in range(1, X)]

    near = [(0, 0)] + [(0, i) for i in range(1, X)] + [(j, 0) for j in range(1, Y)]
    mrows = tile * rows
    per_core = Z // tile

    def product(n, held, group):
        cc, zt = n // per_core, n % per_core
        total = None
        for j, i in group:
            o = fs_at(j, i)
            a = nrm[cc, pl.ds(zt * tile, tile), :, pl.ds(pl.multiple_of(o * K, K), K)].reshape(mrows, K)
            p = lax.dot_general(a, held[o], (((1,), (1,)), ((), ())), preferred_element_type=F32)
            total = p if total is None else total + p
        return total

    def gate_near(n):
        acc_g[n] = product(n, Wg, near)

    phase_one((0, 1))
    if R:
        pl.when(edge)(lambda: over_in().start())
    for a in range(strips):
        part_rows = pl.ds(a * strip, strip)
        values = tok_v[part_rows, :].astype(F32)
        factor = lax.rsqrt(jnp.mean(values * values, axis=-1, keepdims=True) + eps_floor)
        nrm[c, z, part_rows] = (values * factor * gain_v[...]).astype(BF16)
        for direction in range(2):
            cp, ok = tok_chain(direction, 0, a)
            pl.when(ok)(cp.start)
        if C > 1:
            tok_sib(z, a).start()
    if R:
        @pl.when(inner)
        def _():
            pltpu.make_async_copy(over.at[f], over.at[f], over_recv).wait()
            phase_one((4,))
            phase_own((4,))
    phase_own((0, 1))
    if R:
        @pl.when(jnp.logical_not(edge))
        def _():
            phase_one((3,))
            phase_own((3,))
    if Z > 1:
        for a in range(strips):
            tok_arrive(1, a)
    if Z > 2:
        tok_arrive(2, 0)
    if R:
        pl.when(inner)(over_relay)
    phase_relay((0, 1))
    if Z > 2:
        for a in range(1, strips):
            tok_arrive(2, a)
    if R:
        pl.when(inner)(over_cross)
        pl.when(jnp.logical_not(edge))(lambda: phase_relay((3,)))
    if C > 1:
        ref = nrm.at[sib, pl.ds(home * tile, tile)]
        pltpu.make_async_copy(ref, ref, ts_recv.at[0]).wait()
    wait_cross((0,))

    @pl.loop(0, C)
    def _(cc):
        gate_near(cc * per_core + home)

    for s in range(3, Z):
        for a in range(strips):
            tok_arrive(s, a)
    for h in range(cuts):
        down_send(h)
    if R:
        pl.when(inner)(over_diag)
    if C > 1 and per_core > 1:
        ref = nrm.at[sib, pl.ds(0, Z - tile)]
        pltpu.make_async_copy(ref, ref, ts_recv.at[1]).wait()

    if per_core > 1:
        @pl.loop(0, C * (per_core - 1))
        def _(k):
            gate_near(k // (per_core - 1) * per_core + lax.rem(home + 1 + k % (per_core - 1), per_core))

    wait_diag((0,))

    @pl.loop(0, C * per_core)
    def _(n):
        g = acc_g[n]
        if far:
            g = g + product(n, Wg, far)
        acc_g[n] = jax.nn.silu(g)

    if R:
        pl.when(edge)(edge_direct)
    wait_cross(ups)

    @pl.loop(0, C * per_core)
    def _(n):
        acc_u[n] = product(n, Wu, near)

    wait_diag(ups)

    @pl.loop(0, C * per_core)
    def _(n):
        u = acc_u[n]
        if far:
            u = u + product(n, Wu, far)
        hid[n // per_core, pl.ds((n % per_core) * tile, tile)] = (acc_g[n] * u).astype(BF16).reshape(tile, rows, H)

    def sum_slot(direction, d, at):
        return d if direction == 0 else jnp.where(at == d, Z, d)

    units = []

    def spot(ref, q, *at):
        return ref.at[(q, *at)]

    def sum_copy(q, direction, d):
        to = above if direction == 0 else below
        return pltpu.make_async_remote_copy(
            src_ref=spot(rs_s, q, d), dst_ref=spot(rs_r, q, direction, d),
            send_sem=q_send, recv_sem=q_recv.at[q, sum_slot(direction, d, to)],
            device_id={"tp": tp_at(to, c)}, device_id_type=MESH)

    def sum_wait(q, direction, d):
        ref = spot(rs_r, q, direction, d)
        pltpu.make_async_copy(ref, ref, q_recv.at[q, sum_slot(direction, d, z)]).wait()

    def add_sib(q, d):
        if C > 1:
            ref = spot(part, q, d)
            ref[...] = ref[...] + spot(sib_r, q, d)[...].astype(F32)

    def open_sum(qs, direction, order):
        for d in order:
            for q in qs:
                total = spot(part, q, d)[...]
                if C > 1:
                    total = total + spot(sib_r, q, d)[...].astype(F32)
                spot(rs_s, q, d)[...] = total.astype(BF16)
                sum_copy(q, direction, d).start()

    def settle(qs, hold, held):
        def ends(direction, order):
            open_sum(qs, direction, order[:1])
            if not hold:
                open_sum(held + qs, direction, order[1:])

        if Z > 1:
            pl.when(z == 0)(lambda: ends(0, list(range(Z - 1, 0, -1))))
            pl.when(z == Z - 1)(lambda: ends(1, list(range(Z - 1))))

        @pl.loop(0, Z)
        def _(d):
            @pl.when(jnp.logical_or(d == z, jnp.logical_and(z > 0, z < Z - 1)))
            def _():
                for q in qs:
                    add_sib(q, d)

    def down(new, apart=False, hold=False, held=()):
        qs = list(range(len(units), len(units) + len(new)))
        units.extend(new)

        def times(of, q):
            j, i, h = units[q]
            return jnp.dot(hid[of].reshape(Z * rows, H), Wd[fs_at(j, i), :, h * N:(h + 1) * N],
                           preferred_element_type=F32)

        copies = []
        if C > 1:
            for q in qs:
                ref = spot(sib_s, q, slice(None))
                ref[...] = times(sib, q).astype(BF16).reshape(ref.shape)
                cp = pltpu.make_async_remote_copy(
                    src_ref=ref, dst_ref=spot(sib_r, q, slice(None)), send_sem=p_send, recv_sem=p_recv.at[q],
                    device_id={"tp": tp_at(z, sib)}, device_id_type=MESH)
                cp.start()
                copies.append(cp)
        for k, q in enumerate(qs):
            ref = spot(part, q, slice(None))
            ref[...] = times(c, q).reshape(ref.shape)
            if C > 1:
                copies[k].wait_recv()
            if apart:
                settle([q], hold, [])
        if not apart:
            settle(qs, hold, list(held))
        return qs

    low = 2 * z < Z

    def sum_step(q, direction, d, ok):
        @pl.when(ok)
        def _():
            sum_wait(q, direction, d)
            total = spot(part, q, d)[...] + spot(rs_r, q, direction, d)[...].astype(F32)
            spot(rs_s, q, d)[...] = total.astype(BF16)
            sum_copy(q, direction, d).start()

    def near_low(q, k):
        d = Z - 1 - k
        sum_step(q, 0, d, jnp.logical_and(jnp.logical_and(z > 0, z < d), low))

    def near_high(q, k):
        sum_step(q, 1, k, jnp.logical_and(jnp.logical_and(z < Z - 1, z > k), jnp.logical_not(low)))

    def far_low(q, k):
        sum_step(q, 1, k, jnp.logical_and(z > k, low))

    def far_high(q, k):
        d = Z - 1 - k
        sum_step(q, 0, d, jnp.logical_and(z < d, jnp.logical_not(low)))

    hops = range(Z - 1)

    def sum_near(qs, ks=hops):
        for k in ks:
            for q in qs:
                near_low(q, k)
                near_high(q, k)

    def sum_far(qs):
        for k in hops:
            for q in qs:
                far_low(q, k)
                far_high(q, k)

    def sum_end(q):
        j, i, h = units[q]
        mine = spot(part, q, z)
        for direction, there in ((0, z > 0), (1, z < Z - 1)):
            @pl.when(there)
            def _():
                sum_wait(q, direction, z)
                mine[...] = mine[...] + spot(rs_r, q, direction, z)[...].astype(F32)

        col = pl.multiple_of((fs_at(j, i) * cuts + h) * N, N)
        out[:, pl.ds(col, N)] = mine[...].astype(BF16)

    both = range(cuts)
    first, rest = hops[:1], hops[1:]
    groups = [down([(0, 0, h) for h in both], True)]
    sum_near(groups[0])
    for h in both:
        last = h == cuts - 1
        down_relay(h)
        groups.append(down([(j, i, h) for j, i in in_row + in_col], hold=last))
        sum_near(groups[-1], first if last else hops)
        sum_far(groups[-2])
    tail = groups[-1:]
    for h in both:
        down_diag(h)
        tail.append(down([(j, i, h) for j, i in far], hold=h < cuts - 1, held=sum(tail, [])))
        sum_near(tail[-1], first)
    for qs in groups[:-1]:
        for q in qs:
            sum_end(q)
    for qs in tail:
        sum_far(qs)
        sum_near(qs, rest)
    for qs in tail:
        for q in qs:
            sum_end(q)

    def sent(ref, sem):
        pltpu.make_async_copy(ref, ref, sem).wait()

    if F > 1:
        most = pl.ds(0, F - 1)
        sent(Wg.at[most], w_send.at[0])
        sent(Wu.at[most, pl.ds(0, 2 * n0)], w_send.at[1])
        sent(Wd.at[most], w_send.at[2])
        if R:
            pl.when(jnp.logical_not(edge))(lambda: sent(Wu.at[most, pl.ds(2 * n0, 2 * R)], w_send.at[3]))

            @pl.when(inner)
            def _():
                sent(over.at[most], w_send.at[4])
                sent(over.at[most], w_send.at[5])
    if R:
        pl.when(edge)(lambda: sent(over.at[f], w_send.at[3]))
    for k in range(Z):
        if k < Z - 1:
            pl.when(z == k)(lambda: sent(nrm.at[c, pl.ds(0, k + 1)], t_send.at[0]))
        if k > 0:
            pl.when(z == k)(lambda: sent(nrm.at[c, pl.ds(k, Z - k)], t_send.at[1]))
    if C > 1:
        sent(nrm.at[c], ts_send)
        sent(sib_s, p_send)
    if Z > 1:
        sent(rs_s.at[:, pl.ds(0, Z - 1)], q_send)


def local(sizes, tokens, norm_gain, gate_weight, up_weight, down_weight):
    Y, X, Z, C = sizes
    F = Y * X
    rows, D = tokens.shape
    gate_weight, up_weight = gate_weight.T, up_weight.T
    H, K = gate_weight.shape
    cuts = 2 if down_weight.shape[1] % 256 == 0 else 1
    N = down_weight.shape[1] // cuts
    U = F * cuts
    tile = 2 if Z % 2 == 0 else 1
    R = max(H * 3 // 44 // 16, 1) * 16 if Z >= 4 and F > 1 and H % 32 == 0 else 0
    strips = 2 if rows % 32 == 0 else 1
    vmem = pl.BlockSpec(memory_space=pltpu.VMEM)
    dma = pltpu.SemaphoreType.DMA
    hbm = pl.BlockSpec(memory_space=pl.ANY)
    return pl.pallas_call(
        functools.partial(kernel, Y, X, Z, C, cuts, R),
        out_shape=pltpu.VMEM((rows, D), BF16),
        in_specs=[hbm] * 5,
        out_specs=vmem,
        scratch_shapes=[
            pltpu.VMEM((C, Z, rows, D), BF16),
            pltpu.VMEM((F, H, K), BF16),
            pltpu.VMEM((F, H, K), BF16),
            pltpu.VMEM((F, H, N * cuts), BF16),
            pltpu.VMEM((F, 2 * max(R, 8), K), BF16),
            pltpu.VMEM((C * Z // tile, tile * rows, H), F32),
            pltpu.VMEM((C * Z // tile, tile * rows, H), F32),
            pltpu.VMEM((C, Z, rows, H), BF16),
            pltpu.VMEM((U, Z, rows, N), BF16),
            pltpu.VMEM((U, Z, rows, N), BF16),
            pltpu.VMEM((U, Z, rows, N), BF16),
            pltpu.VMEM((U, 2, Z, rows, N), BF16),
            pltpu.VMEM((U, Z, rows, N), F32),
            pltpu.VMEM((rows, D), BF16),
            pltpu.VMEM((1, D), F32),
            dma((5,)),
            dma((6,)), dma((7, 2, max(F - 1, 1))), dma,
            dma((2,)), dma((2, max(Z - 1, 1), strips)), dma, dma((2,)),
            dma, dma((U,)), dma, dma((U, Z + 1)),
        ],
        compiler_params=pltpu.CompilerParams(
            collective_id=0, has_side_effects=True, vmem_limit_bytes=60 * 1024 * 1024),
    )(tokens, norm_gain.reshape(1, D), gate_weight, up_weight, down_weight)


def solution(mesh):
    fs, tp = mesh.shape["fs"], mesh.shape["tp"]
    X = max(n for n in range(1, math.isqrt(fs) + 1) if fs % n == 0)
    C = 2 if tp % 2 == 0 else 1
    from jax.sharding import PartitionSpec as P
    return jax.shard_map(
        functools.partial(local, (fs // X, X, tp // C, C)),
        mesh=mesh,
        in_specs=(P(("fs", "tp"), None), P(), P("fs", "tp"), P("fs", "tp"), P("tp", "fs")),
        out_specs=P(("fs", "tp"), None),
        check_vma=False,
    )
```

```python
import functools
import math

import jax
import jax.numpy as jnp
from jax import lax
from jax.experimental import pallas as pl
from jax.experimental.pallas import tpu as pltpu

eps_floor = 0.05
MESH = pl.DeviceIdType.MESH
F32 = jnp.float32
BF16 = jnp.bfloat16


def kernel(Y, X, Z, C, cuts, R, tok, gain, gw, uw, dw, out, nrm, Wg, Wu, Wd, over, acc_g, acc_u, hid,
           sib_s, sib_r, rs_s, rs_r, part, tok_v, gain_v, w_local,
           w_send, w_recv, over_recv, t_send, t_recv, ts_send, ts_recv, p_send, p_recv, q_send, q_recv):
    F = Y * X
    f = lax.axis_index("fs")
    t = lax.axis_index("tp")
    y, x = f // X, f % X
    z, c = t // C, t % C
    rows, D = tok.shape
    H, K = gw.shape
    N = dw.shape[1] // cuts
    tile = 2 if Z % 2 == 0 else 1
    n0 = H // 2 - R
    strips = 2 if rows % 32 == 0 else 1
    strip = rows // strips
    ups = (1, 3) if R else (1,)
    halves = (5, 6)
    home = z // tile
    edge = jnp.logical_or(z == 0, z == Z - 1)
    inner = jnp.logical_or(z == 1, z == Z - 2)

    def fs_at(j, i):
        return lax.rem(y + j, Y) * X + lax.rem(x + i, X)

    def tp_at(zz, cc):
        return zz * C + cc

    sib = lax.rem(c + 1, C)

    barrier = pltpu.get_barrier_semaphore()
    peers = [{"fs": fs_at(0, i)} for i in range(1, X)] + [{"fs": fs_at(j, 0)} for j in range(1, Y)]
    if C > 1:
        peers += [{"tp": tp_at(z, sib)}]

    def greet(peer):
        pl.semaphore_signal(barrier, inc=1, device_id=peer, device_id_type=MESH)

    for peer in peers:
        greet(peer)
    below, above = jnp.maximum(z - 1, 0), jnp.minimum(z + 1, Z - 1)
    pl.when(z > 0)(lambda: greet({"tp": tp_at(below, c)}))
    pl.when(z < Z - 1)(lambda: greet({"tp": tp_at(above, c)}))

    mats = ((gw, Wg), (uw, Wu), (dw, Wd))
    own_copies = [pltpu.make_async_copy(ref, held.at[f], w_local.at[m]) for m, (ref, held) in enumerate(mats)]
    own_copies += [pltpu.make_async_copy(tok, tok_v, w_local.at[3]), pltpu.make_async_copy(gain, gain_v, w_local.at[4])]
    for cp in own_copies:
        cp.start()

    pl.semaphore_wait(barrier, len(peers) + (z > 0).astype(jnp.int32) + (z < Z - 1).astype(jnp.int32))
    for cp in own_copies:
        cp.wait()

    def piece(m, h, j, i):
        o = fs_at(j, i)
        if m == 0:
            return Wg.at[o, pl.ds(h * (H // 2), H // 2)]
        if m == 1:
            return Wu.at[o, pl.ds(h * n0, n0)]
        if m == 3:
            return Wu.at[o, pl.ds(2 * n0 + h * R, R)]
        if m == 4:
            return over.at[o, pl.ds(h * R, R)]
        if m in (5, 6):
            return Wd.at[o, pl.ds((m - 5) * (H // 2), H // 2), pl.ds(h * N, N)]
        return Wd.at[o, :, pl.ds(h * N, N)]

    def w_copy(m, h, j, i, dj, di):
        slot = ((j - dj) % Y) * X + (i - di) % X
        cp = pltpu.make_async_remote_copy(
            src_ref=piece(m, h, j, i), dst_ref=piece(m, h, j, i),
            send_sem=w_send.at[2 if m in halves else m], recv_sem=w_recv.at[m, h, slot - 1],
            device_id={"fs": fs_at(dj, di)}, device_id_type=MESH)
        cp.start()

    def w_wait(m, h, j, i):
        ref = piece(m, h, j, i)
        pltpu.make_async_copy(ref, ref, w_recv.at[m, h, j * X + i - 1]).wait()

    def phase_one(ms):
        for m in ms:
            for i in range(1, X):
                w_copy(m, 0, 0, 0, 0, i)
            for j in range(1, Y):
                w_copy(m, 1, 0, 0, j, 0)

    def phase_own(ms):
        for m in ms:
            for i in range(1, X):
                w_copy(m, 1, 0, 0, 0, i)
            for j in range(1, Y):
                w_copy(m, 0, 0, 0, j, 0)

    def phase_relay(ms):
        for m in ms:
            for i in range(1, X):
                w_wait(m, 0, 0, i)
                for j in range(1, Y):
                    w_copy(m, 0, 0, i, j, 0)
            for j in range(1, Y):
                w_wait(m, 1, j, 0)
                for i in range(1, X):
                    w_copy(m, 1, j, 0, 0, i)

    def down_send(h):
        for i in range(1, X):
            w_copy(2, h, 0, 0, 0, i)
        for j in range(1, Y):
            w_copy(2, h, 0, 0, j, 0)

    def down_relay(h):
        for i in range(1, X):
            w_wait(2, h, 0, i)
            for j in range(1, Y):
                w_copy(5, h, 0, i, j, 0)
        for j in range(1, Y):
            w_wait(2, h, j, 0)
            for i in range(1, X):
                w_copy(6, h, j, 0, 0, i)

    def down_diag(h):
        for j, i in far:
            w_wait(5, h, j, i)
            w_wait(6, h, j, i)

    def wait_cross(ms):
        for m in ms:
            for i in range(1, X):
                w_wait(m, 1, 0, i)
            for j in range(1, Y):
                w_wait(m, 0, j, 0)

    def wait_diag(ms):
        for m in ms:
            for j in range(1, Y):
                for i in range(1, X):
                    w_wait(m, 0, j, i)
                    w_wait(m, 1, j, i)

    def over_in():
        o = fs_at(0, 0)
        to = jnp.where(z == 0, 1, Z - 2)
        return pltpu.make_async_remote_copy(
            src_ref=Wu.at[o, pl.ds(2 * n0, 2 * R)], dst_ref=over.at[o],
            send_sem=w_send.at[3], recv_sem=over_recv,
            device_id={"tp": tp_at(to, c)}, device_id_type=MESH)

    def over_out(group):
        to = jnp.where(z == 1, 0, Z - 1)
        for j, i in group:
            for h in range(2):
                pltpu.make_async_remote_copy(
                    src_ref=piece(4, h, j, i), dst_ref=piece(3, h, j, i),
                    send_sem=w_send.at[5], recv_sem=w_recv.at[3, h, j * X + i - 1],
                    device_id={"tp": tp_at(to, c)}, device_id_type=MESH).start()

    def tok_chain(direction, s, a):
        src = z - s if direction == 0 else z + s
        dst = z + 1 if direction == 0 else z - 1
        ok = jnp.logical_and(src >= 0, dst < Z) if direction == 0 else jnp.logical_and(src < Z, dst >= 0)
        src, dst = jnp.clip(src, 0, Z - 1), jnp.clip(dst, 0, Z - 1)
        ref = nrm.at[c, src, pl.ds(a * strip, strip)]
        cp = pltpu.make_async_remote_copy(
            src_ref=ref, dst_ref=ref,
            send_sem=t_send.at[direction], recv_sem=t_recv.at[direction, s, a],
            device_id={"tp": tp_at(dst, c)}, device_id_type=MESH)
        return cp, ok

    def tok_sib(zz, a):
        ref = nrm.at[c, zz, pl.ds(a * strip, strip)]
        return pltpu.make_async_remote_copy(
            src_ref=ref, dst_ref=ref,
            send_sem=ts_send, recv_sem=ts_recv.at[jnp.where(zz // tile == home, 0, 1)],
            device_id={"tp": tp_at(z, sib)}, device_id_type=MESH)

    def tok_arrive(s, a):
        for direction in range(2):
            src = z - s if direction == 0 else z + s
            there = src >= 0 if direction == 0 else src < Z
            src = jnp.clip(src, 0, Z - 1)

            @pl.when(there)
            def _():
                ref = nrm.at[c, src, pl.ds(a * strip, strip)]
                pltpu.make_async_copy(ref, ref, t_recv.at[direction, s - 1, a]).wait()
                if C > 1:
                    tok_sib(src, a).start()

            if s < Z - 1:
                cp, ok = tok_chain(direction, s, a)
                pl.when(ok)(cp.start)

    def over_relay():
        for i in range(1, X):
            w_wait(4, 0, 0, i)
            for j in range(1, Y):
                w_copy(4, 0, 0, i, j, 0)
        for j in range(1, Y):
            w_wait(4, 1, j, 0)
            for i in range(1, X):
                w_copy(4, 1, j, 0, 0, i)

    def edge_direct():
        for i in range(1, X):
            w_wait(3, 0, 0, i)
        for j in range(1, Y):
            w_wait(3, 1, j, 0)

    def over_cross():
        wait_cross((4,))
        over_out(in_row + in_col)

    def over_diag():
        wait_diag((4,))
        over_out(far)

    in_row = [(0, i) for i in range(1, X)]
    in_col = [(j, 0) for j in range(1, Y)]
    far = [(j, i) for j in range(1, Y) for i in range(1, X)]

    near = [(0, 0)] + [(0, i) for i in range(1, X)] + [(j, 0) for j in range(1, Y)]
    mrows = tile * rows
    per_core = Z // tile

    def product(n, held, group):
        cc, zt = n // per_core, n % per_core
        total = None
        for j, i in group:
            o = fs_at(j, i)
            a = nrm[cc, pl.ds(zt * tile, tile), :, pl.ds(pl.multiple_of(o * K, K), K)].reshape(mrows, K)
            p = lax.dot_general(a, held[o], (((1,), (1,)), ((), ())), preferred_element_type=F32)
            total = p if total is None else total + p
        return total

    def gate_near(n):
        acc_g[n] = product(n, Wg, near)

    phase_one((0, 1))
    if R:
        pl.when(edge)(lambda: over_in().start())
    for a in range(strips):
        part_rows = pl.ds(a * strip, strip)
        values = tok_v[part_rows, :].astype(F32)
        factor = lax.rsqrt(jnp.mean(values * values, axis=-1, keepdims=True) + eps_floor)
        nrm[c, z, part_rows] = (values * factor * gain_v[...]).astype(BF16)
        for direction in range(2):
            cp, ok = tok_chain(direction, 0, a)
            pl.when(ok)(cp.start)
        if C > 1:
            tok_sib(z, a).start()
    if R:
        @pl.when(inner)
        def _():
            pltpu.make_async_copy(over.at[f], over.at[f], over_recv).wait()
            phase_one((4,))
            phase_own((4,))
    phase_own((0, 1))
    if R:
        @pl.when(jnp.logical_not(edge))
        def _():
            phase_one((3,))
            phase_own((3,))
    if Z > 1:
        for a in range(strips):
            tok_arrive(1, a)
    if Z > 2:
        tok_arrive(2, 0)
    if R:
        pl.when(inner)(over_relay)
    phase_relay((0, 1))
    if Z > 2:
        for a in range(1, strips):
            tok_arrive(2, a)
    if R:
        pl.when(inner)(over_cross)
        pl.when(jnp.logical_not(edge))(lambda: phase_relay((3,)))
    if C > 1:
        ref = nrm.at[sib, pl.ds(home * tile, tile)]
        pltpu.make_async_copy(ref, ref, ts_recv.at[0]).wait()
    wait_cross((0,))

    @pl.loop(0, C)
    def _(cc):
        gate_near(cc * per_core + home)

    for s in range(3, Z):
        for a in range(strips):
            tok_arrive(s, a)
    for h in range(cuts):
        down_send(h)
    if R:
        pl.when(inner)(over_diag)
    if C > 1 and per_core > 1:
        ref = nrm.at[sib, pl.ds(0, Z - tile)]
        pltpu.make_async_copy(ref, ref, ts_recv.at[1]).wait()

    if per_core > 1:
        @pl.loop(0, C * (per_core - 1))
        def _(k):
            gate_near(k // (per_core - 1) * per_core + lax.rem(home + 1 + k % (per_core - 1), per_core))

    wait_diag((0,))

    @pl.loop(0, C * per_core)
    def _(n):
        g = acc_g[n]
        if far:
            g = g + product(n, Wg, far)
        acc_g[n] = jax.nn.silu(g)

    if R:
        pl.when(edge)(edge_direct)
    wait_cross(ups)

    @pl.loop(0, C * per_core)
    def _(n):
        acc_u[n] = product(n, Wu, near)

    wait_diag(ups)

    @pl.loop(0, C * per_core)
    def _(n):
        u = acc_u[n]
        if far:
            u = u + product(n, Wu, far)
        hid[n // per_core, pl.ds((n % per_core) * tile, tile)] = (acc_g[n] * u).astype(BF16).reshape(tile, rows, H)

    def sum_slot(direction, d, at):
        return d if direction == 0 else jnp.where(at == d, Z, d)

    units = []

    def spot(ref, q, *at):
        return ref.at[(q, *at)]

    def sum_copy(q, direction, d):
        to = above if direction == 0 else below
        return pltpu.make_async_remote_copy(
            src_ref=spot(rs_s, q, d), dst_ref=spot(rs_r, q, direction, d),
            send_sem=q_send, recv_sem=q_recv.at[q, sum_slot(direction, d, to)],
            device_id={"tp": tp_at(to, c)}, device_id_type=MESH)

    def sum_wait(q, direction, d):
        ref = spot(rs_r, q, direction, d)
        pltpu.make_async_copy(ref, ref, q_recv.at[q, sum_slot(direction, d, z)]).wait()

    def add_sib(q, d):
        if C > 1:
            ref = spot(part, q, d)
            ref[...] = ref[...] + spot(sib_r, q, d)[...].astype(F32)

    def open_sum(qs, direction, order):
        for d in order:
            for q in qs:
                total = spot(part, q, d)[...]
                if C > 1:
                    total = total + spot(sib_r, q, d)[...].astype(F32)
                spot(rs_s, q, d)[...] = total.astype(BF16)
                sum_copy(q, direction, d).start()

    def settle(qs, hold, held):
        def ends(direction, order):
            open_sum(qs, direction, order[:1])
            if not hold:
                open_sum(held + qs, direction, order[1:])

        if Z > 1:
            pl.when(z == 0)(lambda: ends(0, list(range(Z - 1, 0, -1))))
            pl.when(z == Z - 1)(lambda: ends(1, list(range(Z - 1))))

        @pl.loop(0, Z)
        def _(d):
            @pl.when(jnp.logical_or(d == z, jnp.logical_and(z > 0, z < Z - 1)))
            def _():
                for q in qs:
                    add_sib(q, d)

    def times(of, q, at=slice(None)):
        j, i, h = units[q]
        a = hid[of, at]
        p = jnp.dot(a.reshape(-1, H), Wd[fs_at(j, i), :, h * N:(h + 1) * N], preferred_element_type=F32)
        return p.reshape(*a.shape[:-1], N)

    def pass_sib(q, sem, at=slice(None)):
        ref = spot(sib_s, q, at)
        ref[...] = times(sib, q, at).astype(BF16)
        cp = pltpu.make_async_remote_copy(
            src_ref=ref, dst_ref=spot(sib_r, q, at), send_sem=p_send, recv_sem=p_recv.at[sem],
            device_id={"tp": tp_at(z, sib)}, device_id_type=MESH)
        cp.start()
        return cp

    def down(new, apart=False, hold=False, held=()):
        qs = list(range(len(units), len(units) + len(new)))
        units.extend(new)

        copies = []
        if C > 1:
            copies = [pass_sib(q, q) for q in qs]
        for k, q in enumerate(qs):
            ref = spot(part, q, slice(None))
            ref[...] = times(c, q)
            if C > 1:
                copies[k].wait_recv()
            if apart:
                settle([q], hold, [])
        if not apart:
            settle(qs, hold, list(held))
        return qs

    low = 2 * z < Z

    def sum_step(q, direction, d, ok):
        @pl.when(ok)
        def _():
            sum_wait(q, direction, d)
            total = spot(part, q, d)[...] + spot(rs_r, q, direction, d)[...].astype(F32)
            spot(rs_s, q, d)[...] = total.astype(BF16)
            sum_copy(q, direction, d).start()

    def near_low(q, k):
        d = Z - 1 - k
        sum_step(q, 0, d, jnp.logical_and(jnp.logical_and(z > 0, z < d), low))

    def near_high(q, k):
        sum_step(q, 1, k, jnp.logical_and(jnp.logical_and(z < Z - 1, z > k), jnp.logical_not(low)))

    def far_low(q, k):
        sum_step(q, 1, k, jnp.logical_and(z > k, low))

    def far_high(q, k):
        d = Z - 1 - k
        sum_step(q, 0, d, jnp.logical_and(z < d, jnp.logical_not(low)))

    hops = range(Z - 1)

    def sum_near(qs, ks=hops):
        for k in ks:
            for q in qs:
                near_low(q, k)
                near_high(q, k)

    def sum_far(qs):
        for k in hops:
            for q in qs:
                far_low(q, k)
                far_high(q, k)

    def eager(new, sem, held=(), between=lambda: None):
        if C == 1 or Z == 1:
            q, = down([new], held=held)
            sum_near([q], hops[:1])
            return [q]
        q = len(units)
        units.append(new)
        tip = jnp.where(low, Z - 1, 0)
        others = pl.ds(jnp.where(low, 0, 1), Z - 1)
        tip_in = pass_sib(q, q, tip)
        spot(part, q, tip)[...] = times(c, q, tip)

        def settle_tip():
            tip_in.wait_recv()
            pl.when(z == 0)(lambda: open_sum([q], 0, [Z - 1]))
            pl.when(z == Z - 1)(lambda: open_sum([q], 1, [0]))
            pl.when(jnp.logical_and(z > 0, z < Z - 1))(lambda: add_sib(q, tip))
            near_low(q, 0)
            near_high(q, 0)

        pl.when(c == 0)(settle_tip)
        others_in = pass_sib(q, sem, others)
        pl.when(c > 0)(settle_tip)
        between()
        spot(part, q, others)[...] = times(c, q, others)
        others_in.wait_recv()
        pl.when(z == 0)(lambda: open_sum(list(held) + [q], 0, range(Z - 2, 0, -1)))
        pl.when(z == Z - 1)(lambda: open_sum(list(held) + [q], 1, range(1, Z - 1)))

        @pl.loop(0, Z)
        def _(d):
            @pl.when(jnp.logical_and(d != tip, jnp.logical_or(d == z, jnp.logical_and(z > 0, z < Z - 1))))
            def _():
                add_sib(q, d)
        return [q]

    def sum_end(q):
        j, i, h = units[q]
        mine = spot(part, q, z)
        for direction, there in ((0, z > 0), (1, z < Z - 1)):
            @pl.when(there)
            def _():
                sum_wait(q, direction, z)
                mine[...] = mine[...] + spot(rs_r, q, direction, z)[...].astype(F32)

        col = pl.multiple_of((fs_at(j, i) * cuts + h) * N, N)
        out[:, pl.ds(col, N)] = mine[...].astype(BF16)

    both = range(cuts)
    first, rest = hops[:1], hops[1:]
    tail = []
    qs = eager((0, 0, 0), F * cuts)
    more = down([(0, 0, h) for h in both[1:]])
    sum_near(more, first)
    groups = [qs + more]
    sum_near(groups[0], rest)
    for h in both:
        last = h == cuts - 1
        down_relay(h)
        groups.append(down([(j, i, h) for j, i in in_row + in_col], hold=last))
        sum_near(groups[-1], first if last else hops)
        sum_far(groups[-2])
    tail = groups[-1:]
    for h in both:
        down_diag(h)
        new, held = [(j, i, h) for j, i in far], sum(tail, [])
        if h == cuts - 1 and len(far) == 1:
            tail.append(eager(new[0], F * cuts + 1, held, lambda: sum_far(tail[0])))
        else:
            tail.append(down(new, hold=h < cuts - 1, held=held))
            sum_near(tail[-1], first)
    for qs in groups[:-1]:
        for q in qs:
            sum_end(q)
    for qs in tail:
        if qs is not tail[0] or len(far) != 1:
            sum_far(qs)
        sum_near(qs, rest)
    for qs in tail:
        for q in qs:
            sum_end(q)

    def sent(ref, sem):
        pltpu.make_async_copy(ref, ref, sem).wait()

    if F > 1:
        most = pl.ds(0, F - 1)
        sent(Wg.at[most], w_send.at[0])
        sent(Wu.at[most, pl.ds(0, 2 * n0)], w_send.at[1])
        sent(Wd.at[most], w_send.at[2])
        if R:
            pl.when(jnp.logical_not(edge))(lambda: sent(Wu.at[most, pl.ds(2 * n0, 2 * R)], w_send.at[3]))

            @pl.when(inner)
            def _():
                sent(over.at[most], w_send.at[4])
                sent(over.at[most], w_send.at[5])
    if R:
        pl.when(edge)(lambda: sent(over.at[f], w_send.at[3]))
    for k in range(Z):
        if k < Z - 1:
            pl.when(z == k)(lambda: sent(nrm.at[c, pl.ds(0, k + 1)], t_send.at[0]))
        if k > 0:
            pl.when(z == k)(lambda: sent(nrm.at[c, pl.ds(k, Z - k)], t_send.at[1]))
    if C > 1:
        sent(nrm.at[c], ts_send)
        sent(sib_s, p_send)
    if Z > 1:
        sent(rs_s.at[:, pl.ds(0, Z - 1)], q_send)


def local(sizes, tokens, norm_gain, gate_weight, up_weight, down_weight):
    Y, X, Z, C = sizes
    F = Y * X
    rows, D = tokens.shape
    gate_weight, up_weight = gate_weight.T, up_weight.T
    H, K = gate_weight.shape
    cuts = 2 if down_weight.shape[1] % 256 == 0 else 1
    N = down_weight.shape[1] // cuts
    U = F * cuts
    tile = 2 if Z % 2 == 0 else 1
    R = max(H * 3 // 44 // 16, 1) * 16 if Z >= 4 and F > 1 and H % 32 == 0 else 0
    strips = 2 if rows % 32 == 0 else 1
    vmem = pl.BlockSpec(memory_space=pltpu.VMEM)
    dma = pltpu.SemaphoreType.DMA
    hbm = pl.BlockSpec(memory_space=pl.ANY)
    return pl.pallas_call(
        functools.partial(kernel, Y, X, Z, C, cuts, R),
        out_shape=pltpu.VMEM((rows, D), BF16),
        in_specs=[hbm] * 5,
        out_specs=vmem,
        scratch_shapes=[
            pltpu.VMEM((C, Z, rows, D), BF16),
            pltpu.VMEM((F, H, K), BF16),
            pltpu.VMEM((F, H, K), BF16),
            pltpu.VMEM((F, H, N * cuts), BF16),
            pltpu.VMEM((F, 2 * max(R, 8), K), BF16),
            pltpu.VMEM((C * Z // tile, tile * rows, H), F32),
            pltpu.VMEM((C * Z // tile, tile * rows, H), F32),
            pltpu.VMEM((C, Z, rows, H), BF16),
            pltpu.VMEM((U, Z, rows, N), BF16),
            pltpu.VMEM((U, Z, rows, N), BF16),
            pltpu.VMEM((U, Z, rows, N), BF16),
            pltpu.VMEM((U, 2, Z, rows, N), BF16),
            pltpu.VMEM((U, Z, rows, N), F32),
            pltpu.VMEM((rows, D), BF16),
            pltpu.VMEM((1, D), F32),
            dma((5,)),
            dma((6,)), dma((7, 2, max(F - 1, 1))), dma,
            dma((2,)), dma((2, max(Z - 1, 1), strips)), dma, dma((2,)),
            dma, dma((U + 2,)), dma, dma((U, Z + 1)),
        ],
        compiler_params=pltpu.CompilerParams(
            collective_id=0, has_side_effects=True, vmem_limit_bytes=60 * 1024 * 1024),
    )(tokens, norm_gain.reshape(1, D), gate_weight, up_weight, down_weight)


def solution(mesh):
    fs, tp = mesh.shape["fs"], mesh.shape["tp"]
    X = max(n for n in range(1, math.isqrt(fs) + 1) if fs % n == 0)
    C = 2 if tp % 2 == 0 else 1
    from jax.sharding import PartitionSpec as P
    return jax.shard_map(
        functools.partial(local, (fs // X, X, tp // C, C)),
        mesh=mesh,
        in_specs=(P(("fs", "tp"), None), P(), P("fs", "tp"), P("fs", "tp"), P("tp", "fs")),
        out_specs=P(("fs", "tp"), None),
        check_vma=False,
    )
```
